256 devices in a mesh: ep: 64 (over z, y, core), tp: 4 (over x).
Axes of the slice: x: 4, y: 4, z: 8, core: 2. Of those that a mesh axis runs over, the one named last changes fastest.
Arguments:
- mix_input: bfloat16 [65536, 2048], P(('ep', 'tp')), may hold values from -6 to 6
- mix_gain: float32 [2048], replicated, may hold values from 0.1 to 1.9
- pool_weight: bfloat16 [4, 512, 512], replicated, may hold values from -0.25 to 0.25
- pool_scale: float32 [2048], replicated, may hold values from 0.1 to 1.9
- moe_input: bfloat16 [32768, 2048], P(('ep', 'tp')), may hold values from -6 to 6
- moe_gain: float32 [2048], replicated, may hold values from 0.1 to 1.9
- expert_ids: int32 [32768, 4], P('ep'), may hold values from 0 to 127, all different within a row; in each aligned block of 128 rows (0 to 127, 128 to 255, ...) at most 6 rows name the same one
- route_score: float32 [32768, 4], P(('ep', 'tp')), may hold values from 0.05 to 1
- expert_gate: bfloat16 [128, 2048, 1024], P('ep', None, 'tp'), may hold values from -0.125 to 0.125
- expert_up: bfloat16 [128, 2048, 1024], P('ep', None, 'tp'), may hold values from -0.125 to 0.125
- expert_down: bfloat16 [128, 1024, 2048], P('ep', 'tp'), may hold values from -0.1875 to 0.1875
- shared_gate: bfloat16 [2048, 512], P(None, 'tp'), may hold values from -0.125 to 0.125
- shared_up: bfloat16 [2048, 512], P(None, 'tp'), may hold values from -0.125 to 0.125
- shared_down: bfloat16 [512, 2048], P('tp'), may hold values from -0.25 to 0.25
Outputs:
- mix_output: bfloat16 [65536, 2048], P(('ep', 'tp'))
- moe_output: bfloat16 [32768, 2048], P(('ep', 'tp'))
The draws below stay inside these ranges and needn't reach their ends.
Inputs may be any that keep to these rules, and one draw needn't show every extreme that they name: `expert_ids`: each row names 4 different experts. Within each aligned block of 128 rows (the tokens of one device) no expert is named by more than 6 rows, a bound that some block reaches.
All inputs are finite; a program needn't handle non-finite values.
Results may differ from the reference program's by a relative error of at most 0.012.
Values may be sent and summed in bfloat16 or wider, within the bound.
A program may use at most 192 MiB of HBM per device.

```python
import math
import jax
import jax.numpy as jnp
import numpy as np
from jax import lax

D = 2048
GROUP = 512
FF = 1024
SH = 512
EXPERTS = 128
TOPK = 4
TOK_B = 128
TOKENS_A = 65536
TOKENS_B = 32768
CAP = 6
N_TP = 4


def levels(own_key, dims, shards, least, high):
    factor_of = 1.0
    for dim, blocks in shards:
        draws = jax.random.uniform(jax.random.fold_in(jax.random.fold_in(own_key, 6), dim), (blocks,), jnp.float32, least / len(shards), high / len(shards))
        factor_of = factor_of * jnp.repeat(jnp.exp(draws), dims[dim] // blocks).reshape((-1,) + (1,) * (len(dims) - 1 - dim))
    return factor_of


def routed_block(own_key, own, number, rows, amount, top, most, slope):
    order = jax.random.permutation(own_key, amount)
    packed, ordinary = load_shares(amount, rows * top, most, slope, True), load_shares(amount, rows * top, most, slope, False)
    places = jnp.arange(amount)

    def named(sizes, rotation):
        used = int((sizes > 0).sum())
        fixed = max(1, used // 4)
        moved = fixed + (places - fixed + rotation * (used - fixed)) % max(1, amount - fixed)
        return jnp.zeros((amount,), jnp.int32).at[order[jnp.where(places < fixed, places, moved)]].set(jnp.asarray(sizes, jnp.int32))

    sizes = jnp.where(number % 4 == 0, named(packed, number // 4), named(ordinary, number - number // 4 - 1))
    mixed = jax.random.permutation(jax.random.fold_in(own, 3), amount)
    donor, sink = mixed[0:amount // 2 * 2:2], mixed[1:amount // 2 * 2:2]
    margin = jnp.minimum(sizes[donor] - 1, most - sizes[sink]) // 2
    margin = jnp.where((donor == order[0]) | (sink == order[0]) | (sizes[sink] == 0), 0, jnp.maximum(margin, 0))
    moved = jax.random.randint(jax.random.fold_in(own, 4), (amount // 2,), 0, 1 << 20) % (margin + 1)
    sizes = sizes.at[donor].add(-moved).at[sink].add(moved)
    members = jnp.searchsorted(jnp.cumsum(sizes), jnp.arange(rows * top), side="right").astype(jnp.int32)
    listing = members.reshape(top, rows).T
    listing = listing[jax.random.permutation(jax.random.fold_in(own, 1), rows)]
    rotation = jax.random.randint(jax.random.fold_in(own, 2), (rows, 1), 0, top)
    return jnp.take_along_axis(listing, (jnp.arange(top)[None, :] + rotation) % top, axis=1)


def load_shares(amount, total, most, skew, full):
    weights = [(1 << 20) // math.isqrt(standing ** skew) + 1 for standing in range(1, amount + 1)]
    largest = most if full else min(most, max(-(-total // amount), total * weights[0] // sum(weights)))
    least = 1 if total - largest >= amount - 1 else 0
    given, surplus = [largest] + [least] * (amount - 1), total - largest - least * (amount - 1)
    while surplus > 0:
        movable = [i for i in range(1, amount) if given[i] < largest] or [i for i in range(1, amount) if given[i] < most]
        whole, left = sum([weights[i] for i in movable]), surplus
        for i in movable:
            addition = min(most - given[i], max(1, left * weights[i] // whole), surplus)
            given[i] = given[i] + addition
            surplus = surplus - addition
    return np.array(given)


def scatter_about(rng, shape, scale, bound, pieces=(), held_as=jnp.bfloat16):
    entries = scale * jax.random.normal(rng, shape, jnp.float32)
    if pieces:
        entries = entries * levels(rng, shape, pieces, -0.22, 0.18)
    return jnp.clip(entries, -bound, bound).astype(held_as)


def setup_inputs(seed: int = 0) -> dict:
    splits = jax.random.split(jax.random.key(seed), 15)
    mix_input = scatter_about(splits[0], (TOKENS_A, D), 1.0, 6.0, ((0, 256),))
    mix_gain = jnp.clip(1.0 + 0.18 * jax.random.normal(splits[1], (D,), jnp.float32), 0.1, 1.9)
    pool_weight = scatter_about(splits[2], (4, GROUP, GROUP), GROUP ** -0.5, 0.25)
    pool_scale = jnp.clip(1.0 + 0.18 * jax.random.normal(splits[3], (D,), jnp.float32), 0.1, 1.9)
    moe_input = scatter_about(splits[4], (TOKENS_B, D), 1.0, 6.0, ((0, 256),))
    moe_gain = jnp.clip(1.0 + 0.18 * jax.random.normal(splits[5], (D,), jnp.float32), 0.1, 1.9)
    expert_ids_keys = jax.random.split(jax.random.fold_in(splits[6], 1), TOKENS_B // TOK_B)
    expert_ids_turns = jax.random.permutation(jax.random.fold_in(splits[6], 3), TOKENS_B // TOK_B)
    expert_ids = jax.vmap(lambda own, number: routed_block(jax.random.fold_in(splits[6], 2), own, number, TOK_B, EXPERTS, TOPK, CAP, 1))(expert_ids_keys, expert_ids_turns).reshape((TOKENS_B, TOPK))
    route_score = jnp.clip(jnp.exp(math.log(1.0) - 2.9957323 * jax.random.uniform(splits[7], (TOKENS_B, TOPK), jnp.float32) ** levels(splits[7], (TOKENS_B, TOPK), ((0, 256),), -0.2, 0.2)), 0.05, 1.0)
    expert_gate = scatter_about(splits[8], (EXPERTS, D, FF), D ** -0.5, 0.125, ((0, 64), (2, 4)))
    expert_up = scatter_about(splits[9], (EXPERTS, D, FF), D ** -0.5, 0.125, ((0, 64), (2, 4)))
    expert_down = scatter_about(splits[10], (EXPERTS, FF, D), FF ** -0.5, 0.1875, ((0, 64), (1, 4)))
    shared_gate = scatter_about(splits[11], (D, SH), D ** -0.5, 0.125, ((1, 4),))
    shared_up = scatter_about(splits[12], (D, SH), D ** -0.5, 0.125, ((1, 4),))
    shared_down = scatter_about(splits[13], (SH, D), SH ** -0.5, 0.25, ((0, 4),))
    return dict(mix_input=mix_input, mix_gain=mix_gain, pool_weight=pool_weight, pool_scale=pool_scale, moe_input=moe_input, moe_gain=moe_gain, expert_ids=expert_ids, route_score=route_score, expert_gate=expert_gate, expert_up=expert_up, expert_down=expert_down, shared_gate=shared_gate, shared_up=shared_up, shared_down=shared_down)


WINDOWS = (2, 4, 8, 16)
RMS_EPS = 1e-06
ROUTED_SCALE = 2.5

def rms_norm(values, gain_row):
    upcast = values.astype(jnp.float32)
    scaled = upcast * lax.rsqrt(lax.optimization_barrier(jnp.mean(upcast * upcast, axis=-1, keepdims=True)) + RMS_EPS)
    return (scaled * gain_row).astype(jnp.bfloat16)

def rounded(values):
    return lax.optimization_barrier(values.astype(jnp.bfloat16)).astype(jnp.float32)

def window_means(normed, before, offset):
    row_count = normed.shape[0]
    lead_rows = before.shape[0]
    group_size = normed.shape[1] // len(WINDOWS)
    joined = jnp.concatenate([before, normed], axis=0).astype(jnp.float32)
    positions = offset + jnp.arange(row_count, dtype=jnp.int32)
    window_avg = []
    for group_idx, span in enumerate(WINDOWS):
        channels = joined[:, group_idx * group_size:(group_idx + 1) * group_size]
        first_row = lead_rows - span + 1
        running = channels[first_row:first_row + row_count]
        for shift_idx in range(1, span):
            running = running + channels[first_row + shift_idx:first_row + shift_idx + row_count]
        counts = jnp.minimum(positions + 1, span).astype(jnp.float32)
        window_avg.append(running / counts[:, None])
    return jnp.stack(window_avg, axis=1)

def width_sum(hidden, down_rows, block_width):
    summed = jnp.zeros((hidden.shape[0], down_rows.shape[1]), jnp.float32)
    for part_idx in range(N_TP):
        piece_out = jnp.dot(hidden[:, part_idx * block_width:(part_idx + 1) * block_width], down_rows[part_idx * block_width:(part_idx + 1) * block_width], preferred_element_type=jnp.float32)
        summed = summed + rounded(piece_out)
    return summed.astype(jnp.bfloat16)

def reference(mix_input, mix_gain, pool_weight, pool_scale, moe_input, moe_gain, expert_ids, route_score, expert_gate, expert_up, expert_down, shared_gate, shared_up, shared_down):
    normed = rms_norm(mix_input, mix_gain)
    row_count, width_all = normed.shape
    reach_rows = max(WINDOWS) - 1
    before = jnp.zeros((reach_rows, width_all), jnp.bfloat16)
    pooled = window_means(normed, before, 0)
    difference = (pooled - normed.astype(jnp.float32).reshape(row_count, len(WINDOWS), -1)).astype(jnp.bfloat16)
    mixed_out = jnp.einsum('sgc,gcd->sgd', difference.astype(jnp.float32), pool_weight.astype(jnp.float32))
    mix_output = (mixed_out.reshape(row_count, width_all) * pool_scale).astype(jnp.bfloat16)
    tok_count = moe_input.shape[0]
    h_moe = rms_norm(moe_input, moe_gain)
    block_count = tok_count // TOK_B
    pair_ids = expert_ids.reshape(block_count, TOK_B * TOPK)
    onehot = (pair_ids[:, :, None] == jnp.arange(EXPERTS, dtype=jnp.int32)[None, None, :]).astype(jnp.int32)
    rank = lax.optimization_barrier(jnp.sum((jnp.cumsum(onehot, axis=1) - onehot) * onehot, axis=2))
    block_idx = jnp.arange(block_count, dtype=jnp.int32)[:, None]
    slot_col = block_idx * CAP + rank
    owner = block_idx * TOK_B + jnp.arange(TOK_B * TOPK, dtype=jnp.int32)[None, :] // TOPK
    table = jnp.full((EXPERTS, block_count * CAP), tok_count, jnp.int32).at[pair_ids, slot_col].set(owner)
    padded = jnp.concatenate([h_moe, jnp.zeros((1, D), jnp.bfloat16)], axis=0)

    def run_expert(index):
        picked = padded[table[index]]
        gate_val = jnp.dot(picked, expert_gate[index], preferred_element_type=jnp.float32)
        up_val = jnp.dot(picked, expert_up[index], preferred_element_type=jnp.float32)
        hidden = (jax.nn.silu(gate_val) * up_val).astype(jnp.bfloat16)
        return width_sum(hidden, expert_down[index], FF // N_TP)
    results = lax.map(run_expert, jnp.arange(EXPERTS, dtype=jnp.int32))
    flat_res = results.reshape(EXPERTS * block_count * CAP, D)
    flat_idx = (pair_ids * (block_count * CAP) + slot_col).reshape(tok_count, TOPK)
    shared_gate_val = jnp.dot(h_moe, shared_gate, preferred_element_type=jnp.float32)
    shared_up_val = jnp.dot(h_moe, shared_up, preferred_element_type=jnp.float32)
    shared_hidden = (jax.nn.silu(shared_gate_val) * shared_up_val).astype(jnp.bfloat16)
    shared_out = width_sum(shared_hidden, shared_down, SH // N_TP)
    route_w = route_score / lax.optimization_barrier(jnp.sum(route_score, axis=1, keepdims=True)) * ROUTED_SCALE
    combined = shared_out.astype(jnp.float32)
    for pick_idx in range(TOPK):
        combined = combined + route_w[:, pick_idx:pick_idx + 1] * flat_res[flat_idx[:, pick_idx]].astype(jnp.float32)
    return (mix_output, combined.astype(jnp.bfloat16))
```

```python
import functools

import jax
import jax.numpy as jnp
import numpy as np
from jax import lax
from jax.experimental import pallas as pl
from jax.experimental.pallas import tpu as pltpu
from jax.sharding import PartitionSpec as P

MESH = pl.DeviceIdType.MESH
F32, BF16 = jnp.float32, jnp.bfloat16
WINDOWS = (2, 4, 8, 16)
RMS_EPS = 1e-06
ROUTED_SCALE = 2.5
NZ, NY, NC = 8, 4, 2
COLS = 2
TILE = 256


def rms_norm(values, gain_row):
    upcast = values.astype(F32)
    scaled = upcast * lax.rsqrt(jnp.mean(upcast * upcast, axis=-1, keepdims=True) + RMS_EPS)
    return (scaled * gain_row).astype(BF16)


def dot(a, b):
    return jnp.dot(a, b, preferred_element_type=F32)


def moe_kernel(
    dims,
    x_ref,
    gain_ref,
    meta_ref,
    rep_ref,
    rept_ref,
    tgt_ref,
    tgtt_ref,
    gate_ref,
    up_ref,
    down_ref,
    out_ref,
    hbuf,
    metab,
    pick,
    back,
    wgu,
    wd,
    sendbuf,
    recv,
    xrecv,
    gu,
    psend,
    xback,
    own,
    ret,
    rs_send,
    rs_recv,
    m_sem,
    z_sem,
    ys_sem,
    yr_sem,
    x_sem,
    p_sem,
    r_sem,
    rs_sem,
    wl_sem,
    w_sem,
):
    nz, ny, nx, tok, cap, width = dims
    ring = nz // 2
    peers = ny * NC
    group = nz * cap
    half_rows = peers * group
    rows = 2 * half_rows
    piece = width // COLS
    half = tok // 2
    ep = lax.axis_index("ep")
    tp = lax.axis_index("tp")
    z, q = ep // peers, ep % peers
    y, core = q // NC, q % NC

    def at_z(step):
        return {"ep": ((z + step + nz) % nz) * peers + q}

    def at_peer(dy, dc):
        return {"ep": z * peers + ((y + dy + ny) % ny) * NC + (core + dc + NC) % NC}

    near = tp + 1 - 2 * (tp % 2)
    far = nx - 1 - tp
    weight_side = ({"tp": near}, {"tp": far})
    token_side = ({"tp": far}, {"tp": near})

    barrier = pltpu.get_barrier_semaphore()
    greet = [at_z(1), at_z(-1), {"tp": near}, {"tp": far}]
    greet += [at_peer(r // NC, r % NC) for r in range(1, peers)]
    for device in greet:
        pl.semaphore_signal(barrier, inc=1, device_id=device, device_id_type=MESH)
    pl.semaphore_wait(barrier, len(greet))

    def remote(src, dst, send, recv_, device):
        return pltpu.make_async_remote_copy(
            src_ref=src, dst_ref=dst, send_sem=send, recv_sem=recv_, device_id=device, device_id_type=MESH
        )

    def wait_bytes(ref, sem):
        pltpu.make_async_copy(ref, ref, sem).wait()

    weights = []
    for j in range(2):
        for i, (src, own_dst, far_dst) in enumerate(
            (
                (gate_ref.at[j], wgu.at[j, 0], wgu.at[j, 2]),
                (up_ref.at[j], wgu.at[j, 1], wgu.at[j, 3]),
                (down_ref.at[j], wd.at[j, 0], wd.at[j, 1]),
            )
        ):
            far_copy = remote(src, far_dst, w_sem.at[0, j, i], w_sem.at[1, j, i], weight_side[j])
            own_copy = pltpu.make_async_copy(src, own_dst, wl_sem.at[j, i])
            weights.append((j, far_copy, own_copy))

    hold = rms_norm(x_ref[...], gain_ref[...])
    for g in range(COLS):
        hbuf[g, 0:tok] = hold[:, g * piece : (g + 1) * piece]
    metab[0] = meta_ref[...]

    def meta_copy(d, s):
        src = (-s if d == 0 else s) % nz
        dst = (-s - 1 if d == 0 else s + 1) % nz
        return remote(metab.at[src], metab.at[dst], m_sem.at[0, d, s], m_sem.at[1, d, s], at_z(1 - 2 * d))

    def z_copy(g, d, s, h):
        src = (-s if d == 0 else s) % nz
        dst = (-s - 1 if d == 0 else s + 1) % nz
        return remote(
            hbuf.at[g, pl.ds(src * tok + h * half, half)],
            hbuf.at[g, pl.ds(dst * tok + h * half, half)],
            z_sem.at[0, g, d, s, h],
            z_sem.at[1, g, d, s, h],
            at_z(1 - 2 * d),
        )

    def sends_half(d, s, h):
        return s < ring - 1 or h == d

    def meta_goes(d, s):
        return s < ring - 1 or d == 0

    for d in range(2):
        meta_copy(d, 0).start()
    for h in range(2):
        for d in range(2):
            z_copy(0, d, 0, h).start()
    for j, far_copy, own_copy in weights:
        far_copy.start()
    for j, far_copy, own_copy in weights:
        own_copy.start()

    def z_forward(g, s):
        for h in range(2):
            for d in range(2):
                z_copy(g, d, s - 1, h).wait_recv()
                if sends_half(d, s, h):
                    z_copy(g, d, s, h).start()

    for s in range(1, ring):
        for d in range(2):
            meta_copy(d, s - 1).wait_recv()
            if meta_goes(d, s):
                meta_copy(d, s).start()
    meta_copy(0, ring - 1).wait_recv()

    before = lax.broadcasted_iota(jnp.int32, (tok, tok), 0) < lax.broadcasted_iota(jnp.int32, (tok, tok), 1)
    upper = before.astype(F32).astype(BF16)
    line = lax.broadcasted_iota(jnp.int32, (2 * peers, tok), 0)
    their_core = (core + line % NC) % NC
    their_y = (y + (line % peers) // NC) % ny
    names = (2 * (z * peers + their_y * NC + their_core) + line // peers).astype(F32)

    def tables(zi):
        block = metab[zi].astype(F32)
        named = jnp.zeros((2 * peers, tok), F32)
        weight = jnp.zeros((2 * peers, tok), F32)
        for k in range(4):
            same = (block[k : k + 1] == names).astype(F32)
            named = named + same
            weight = weight + same * block[4 + k : 5 + k]
        rank = dot(named.astype(BF16), upper)
        rank = jnp.where(named > 0.5, rank, -2.0)
        spread = dot(rep_ref[...], rank.astype(BF16))
        pick[:, zi * tok : (zi + 1) * tok] = (spread == tgt_ref[:, zi : zi + 1]).astype(F32).astype(BF16)
        padding = jnp.zeros((tok - 4 * peers, tok), F32)
        turned = jnp.transpose(jnp.concatenate([rank, weight, padding], axis=0))
        spread_t = dot(turned[:, : 2 * peers].astype(BF16), rept_ref[...])
        weight_t = dot(turned[:, 2 * peers : 4 * peers].astype(BF16), rept_ref[...])
        back[zi] = jnp.where(spread_t == tgtt_ref[zi : zi + 1], weight_t, 0.0).astype(BF16)

    for s in range(1, ring):
        z_forward(0, s)
        if s == 1:
            for zi in range(nz):
                tables(zi)
    for g in range(1, COLS):
        for h in range(2):
            for d in range(2):
                z_copy(g, d, 0, h).start()

    def select(g):
        def body(n, _):
            cols = pl.ds(pl.multiple_of(n * TILE, TILE), TILE)
            sendbuf[g, :, cols] = dot(pick[...], hbuf[g, :, cols]).astype(BF16)
            return 0

        lax.fori_loop(0, piece // TILE, body, 0)
        for j in range(2):
            recv[g, j * half_rows : j * half_rows + group] = sendbuf[g, j * half_rows : j * half_rows + group]

    def y_copy(g, j, r):
        part = pl.ds(j * half_rows + r * group, group)
        return remote(
            sendbuf.at[g, part], recv.at[g, part], ys_sem.at[g], yr_sem.at[g, j, r], at_peer(r // NC, r % NC)
        )

    def x_copy(g, j, r):
        part = pl.ds(j * half_rows + r * group, group)
        return remote(recv.at[g, part], xrecv.at[g, part], x_sem.at[0, g, j], x_sem.at[1, g, j], token_side[j])

    order = list(range(1, peers))
    order.sort(key=lambda r: min(r // NC, ny - r // NC))

    def y_start(g):
        for r in order[::-1]:
            for j in range(2):
                y_copy(g, j, r).start()
        for j in range(2):
            x_copy(g, j, 0).start()

    def x_forward(g, some):
        for r in some:
            for j in range(2):
                y_copy(g, j, r).wait_recv()
                x_copy(g, j, r).start()

    def last_z(g):
        for d in range(2):
            z_copy(g, d, ring - 1, d).wait_recv()

    def gate_up(which, g, j):
        src = (recv, xrecv)[which]

        def body(n, _):
            part = dot(src[g, j * half_rows : (j + 1) * half_rows], wgu[j, n, g * piece : (g + 1) * piece])
            if g == 0:
                gu[which, j, n] = part
            else:
                gu[which, j, n] = gu[which, j, n] + part
            return 0

        lax.fori_loop(0, 4, body, 0)

    def hidden(which, j):
        out = []
        for n in (0, 2):
            gate = gu[which, j, n]
            out.append((gate / (1.0 + jnp.exp(-gate)) * gu[which, j, n + 1]).astype(BF16))
        return out

    def down(hid, g, j, dst):
        def body(n, _):
            cols = pl.ds(pl.multiple_of(n * TILE, TILE), TILE)
            wide = pl.ds(pl.multiple_of(g * piece + n * TILE, TILE), TILE)
            dst[g, j, :, cols] = (dot(hid[0], wd[j, 0, :, wide]) + dot(hid[1], wd[j, 1, :, wide])).astype(BF16)
            return 0

        lax.fori_loop(0, piece // TILE, body, 0)

    def p_copy(g, j):
        return remote(psend.at[g, j], xback.at[g, j], p_sem.at[0, g, j], p_sem.at[1, g, j], token_side[j])

    def r_copy(g, j, r):
        return remote(
            own.at[g, j, pl.ds(r * group, group)],
            ret.at[g, pl.ds(j * half_rows + r * group, group)],
            r_sem.at[0, g],
            r_sem.at[1, g],
            at_peer(-(r // NC), -(r % NC)),
        )

    last_z(0)
    select(0)
    y_start(0)
    for s in range(1, ring):
        z_forward(1, s)
        x_forward(0, order[(s - 1) * len(order) // ring : s * len(order) // ring])
    x_forward(0, order[(ring - 1) * len(order) // ring :])
    last_z(1)
    select(1)
    y_start(1)
    for j, far_copy, own_copy in weights:
        own_copy.wait()
        far_copy.wait_recv()
    for j in range(2):
        gate_up(0, 0, j)
    x_forward(1, order)
    for j in range(2):
        wait_bytes(xrecv.at[0, pl.ds(j * half_rows, half_rows)], x_sem.at[1, 0, j])
        gate_up(1, 0, j)
    for j in range(2):
        gate_up(0, 1, j)
    for j in range(2):
        wait_bytes(xrecv.at[1, pl.ds(j * half_rows, half_rows)], x_sem.at[1, 1, j])
        gate_up(1, 1, j)
        hid = hidden(1, j)
        for g in range(COLS):
            down(hid, g, j, psend)
            p_copy(g, j).start()
    for j in range(2):
        hid = hidden(0, j)
        for g in range(COLS):
            down(hid, g, j, own)
    for g in range(COLS):
        for j in range(2):
            p_copy(g, j).wait_recv()
            own[g, j] = (own[g, j].astype(F32) + xback[g, j].astype(F32)).astype(BF16)
            for r in order[::-1]:
                r_copy(g, j, r).start()
            ret[g, j * half_rows : j * half_rows + group] = own[g, j, 0:group]

    def rs_copy(g, d, s):
        part = pl.ds(d * half, half) if s == 0 else pl.ds(0, tok)
        return remote(
            rs_send.at[g, d, s, part],
            rs_recv.at[g, d, s, part],
            rs_sem.at[0, g, d, s],
            rs_sem.at[1, g, d, s],
            at_z(1 - 2 * d),
        )

    def share(g, zi, first, count, adds, dst, dst_at):
        def body(n, _):
            cols = pl.ds(pl.multiple_of(n * TILE, TILE), TILE)
            total = dot(back[zi, first : first + count], ret[g, :, cols])
            for d, s in adds:
                total = total + rs_recv[g, d, s, first : first + count, cols].astype(F32)
            place = pl.ds(pl.multiple_of(dst_at + n * TILE, TILE), TILE)
            if dst is None:
                out_ref[first : first + count, place] = total
            else:
                dst[first : first + count, place] = total.astype(BF16)
            return 0

        lax.fori_loop(0, piece // TILE, body, 0)

    def rs_step(g, s):
        for d in range(2):
            zi = ring - s if d == 0 else ring + s
            dst = rs_send.at[g, d, s]
            if s > 0:
                rs_copy(g, d, s - 1).wait_recv()
            if s == 0:
                share(g, zi, d * half, half, (), dst, 0)
            elif s == 1:
                for h in range(2):
                    share(g, zi, h * half, half, ((d, 0),) if h == d else (), dst, 0)
            else:
                share(g, zi, 0, tok, ((d, s - 1),), dst, 0)
            rs_copy(g, d, s).start()

    def rs_last(g):
        for d in range(2):
            rs_copy(g, d, ring - 1).wait_recv()
        share(g, 0, 0, tok, ((0, ring - 1), (1, ring - 1)), None, g * piece)

    def ret_wait(g):
        far_rows = 2 * (half_rows - group)
        wait_bytes(ret.at[g, pl.ds(0, far_rows)], r_sem.at[1, g])

    ret_wait(0)
    for s in range(ring):
        rs_step(0, s)
        if s == 0:
            ret_wait(1)
        else:
            rs_step(1, s - 1)
    rs_step(1, ring - 1)
    rs_last(0)
    rs_last(1)

    for d in range(2):
        for s in range(ring):
            if meta_goes(d, s):
                meta_copy(d, s).wait_send()
    for g in range(COLS):
        for d in range(2):
            for s in range(ring):
                for h in range(2):
                    if sends_half(d, s, h):
                        z_copy(g, d, s, h).wait_send()
                rs_copy(g, d, s).wait_send()
        far_rows = 2 * (half_rows - group)
        wait_bytes(sendbuf.at[g, pl.ds(0, far_rows)], ys_sem.at[g])
        wait_bytes(ret.at[g, pl.ds(0, far_rows)], r_sem.at[0, g])
        for j in range(2):
            wait_bytes(recv.at[g, pl.ds(0, half_rows)], x_sem.at[0, g, j])
            p_copy(g, j).wait_send()
    for j, far_copy, own_copy in weights:
        far_copy.wait_send()


def routed(dims, moe_input, gain, meta, gate, up, down):
    nz, ny, nx, tok, cap, width = dims
    peers, ring = ny * NC, nz // 2
    group = nz * cap
    half_rows = peers * group
    rows = 2 * half_rows
    piece = width // COLS
    hid = gate.shape[2]
    line = np.arange(rows)
    rep = (line[:, None] // group == np.arange(2 * peers)[None, :]).astype(np.float32)
    turn = (line // cap) % nz
    tgt = np.where(turn[:, None] == np.arange(nz)[None, :], (line % cap)[:, None], -1).astype(np.float32)
    vmem = pl.BlockSpec(memory_space=pltpu.VMEM)
    hbm = pl.BlockSpec(memory_space=pl.ANY)
    dma = pltpu.SemaphoreType.DMA
    return pl.pallas_call(
        functools.partial(moe_kernel, dims),
        out_shape=jax.ShapeDtypeStruct((tok, width), F32),
        in_specs=[vmem] * 7 + [hbm] * 3,
        out_specs=vmem,
        scratch_shapes=[
            pltpu.VMEM((COLS, nz * tok, piece), BF16),
            pltpu.VMEM((nz, 16, tok), BF16),
            pltpu.VMEM((rows, nz * tok), BF16),
            pltpu.VMEM((nz, tok, rows), BF16),
            pltpu.VMEM((2, 4, width, hid), BF16),
            pltpu.VMEM((2, 2, hid, width), BF16),
            pltpu.VMEM((COLS, rows, piece), BF16),
            pltpu.VMEM((COLS, rows, piece), BF16),
            pltpu.VMEM((COLS, rows, piece), BF16),
            pltpu.VMEM((2, 2, 4, half_rows, hid), F32),
            pltpu.VMEM((COLS, 2, half_rows, piece), BF16),
            pltpu.VMEM((COLS, 2, half_rows, piece), BF16),
            pltpu.VMEM((COLS, 2, half_rows, piece), BF16),
            pltpu.VMEM((COLS, rows, piece), BF16),
            pltpu.VMEM((COLS, 2, ring, tok, piece), BF16),
            pltpu.VMEM((COLS, 2, ring, tok, piece), BF16),
            dma((2, 2, ring)),
            dma((2, COLS, 2, ring, 2)),
            dma((COLS,)),
            dma((COLS, 2, peers)),
            dma((2, COLS, 2)),
            dma((2, COLS, 2)),
            dma((2, COLS)),
            dma((2, COLS, 2, ring)),
            dma((2, 3)),
            dma((2, 2, 3)),
        ],
        compiler_params=pltpu.CompilerParams(
            collective_id=0, has_side_effects=True, vmem_limit_bytes=67043328
        ),
        cost_estimate=pl.CostEstimate(flops=40 * 10**9, bytes_accessed=200 * 10**6, transcendentals=0),
    )(
        moe_input,
        gain.reshape(1, width),
        meta,
        jnp.asarray(rep, BF16),
        jnp.asarray(rep.T, BF16),
        jnp.asarray(tgt),
        jnp.asarray(tgt.T),
        gate,
        up,
        down,
    )


def passed_along(value, axis, by):
    length = lax.axis_size(axis)
    pairs = [(i, i + by) for i in range(length) if 0 <= i + by < length]
    return lax.ppermute(value, axis, pairs)


def window_means(normed, before, offset):
    row_count = normed.shape[0]
    lead_rows = before.shape[0]
    group_size = normed.shape[1] // len(WINDOWS)
    joined = jnp.concatenate([before, normed], axis=0).astype(F32)
    positions = offset + jnp.arange(row_count, dtype=jnp.int32)
    window_avg = []
    for group_idx, span in enumerate(WINDOWS):
        channels = joined[:, group_idx * group_size : (group_idx + 1) * group_size]
        first_row = lead_rows - span + 1
        running = channels[first_row : first_row + row_count]
        for shift_idx in range(1, span):
            running = running + channels[first_row + shift_idx : first_row + shift_idx + row_count]
        counts = jnp.minimum(positions + 1, span).astype(F32)
        window_avg.append(running / counts[:, None])
    return jnp.stack(window_avg, axis=1)


def in_one_piece(arrays, axis, dim, along):
    ends, at = ([], 0)
    for a in arrays[:-1]:
        at += a.shape[along]
        ends.append(at)
    both = jnp.concatenate(arrays, axis=along)
    return tuple(jnp.split(lax.all_gather(both, axis, axis=dim, tiled=True), ends, axis=along))


def per_device(
    sizes,
    mix_input,
    mix_gain,
    pool_weight,
    pool_scale,
    moe_input,
    moe_gain,
    expert_ids,
    route_score,
    expert_gate,
    expert_up,
    expert_down,
    shared_gate,
    shared_up,
    shared_down,
):
    nz, ny = sizes
    nx = lax.axis_size("tp")
    tok, width = moe_input.shape
    experts = lax.axis_size("ep") * expert_gate.shape[0]
    cap = 3 * tok * expert_ids.shape[1] // (2 * experts)
    my_ids = lax.dynamic_slice_in_dim(expert_ids, lax.axis_index("tp") * tok, tok, 0)
    route_w = route_score / jnp.sum(route_score, axis=1, keepdims=True) * ROUTED_SCALE
    meta = jnp.concatenate(
        [my_ids.T.astype(BF16), route_w.T.astype(BF16), jnp.zeros((8, tok), BF16)], axis=0
    )
    dims = (nz, ny, nx, tok, cap, width)
    routed_out = routed(dims, moe_input, moe_gain, meta, expert_gate, expert_up, expert_down)

    h_moe = rms_norm(moe_input, moe_gain)
    full_sgate, full_sup = in_one_piece((shared_gate, shared_up), "tp", 1, 0)
    full_sdown = lax.all_gather(shared_down, "tp", axis=0, tiled=True)
    shared_gate_val = dot(h_moe, full_sgate)
    shared_up_val = dot(h_moe, full_sup)
    shared_hidden = (jax.nn.silu(shared_gate_val) * shared_up_val).astype(BF16)
    shared_back = dot(shared_hidden, full_sdown)
    moe_output = (routed_out + shared_back).astype(BF16)

    normed = rms_norm(mix_input, mix_gain)
    row_count, width_all = normed.shape
    reach_rows = max(WINDOWS) - 1
    before = passed_along(normed[row_count - reach_rows :], ("ep", "tp"), 1)
    offset = lax.axis_index(("ep", "tp")) * row_count
    pooled = window_means(normed, before, offset)
    difference = (pooled - normed.astype(F32).reshape(row_count, len(WINDOWS), -1)).astype(BF16)
    mixed_out = jnp.einsum("sgc,gcd->sgd", difference, pool_weight, preferred_element_type=F32)
    mix_output = (mixed_out.reshape(row_count, width_all) * pool_scale).astype(BF16)
    return (mix_output, moe_output)


def solution(mesh, sizes=(NZ, NY)):
    return jax.shard_map(
        functools.partial(per_device, sizes),
        mesh=mesh,
        in_specs=(
            P(("ep", "tp"), None),
            P(),
            P(),
            P(),
            P(("ep", "tp"), None),
            P(),
            P("ep", None),
            P(("ep", "tp"), None),
            P("ep", None, "tp"),
            P("ep", None, "tp"),
            P("ep", "tp", None),
            P(None, "tp"),
            P(None, "tp"),
            P("tp", None),
        ),
        out_specs=(P(("ep", "tp"), None), P(("ep", "tp"), None)),
        check_vma=False,
    )
```

```python
import functools

import jax
import jax.numpy as jnp
import numpy as np
from jax import lax
from jax.experimental import pallas as pl
from jax.experimental.pallas import tpu as pltpu
from jax.sharding import PartitionSpec as P

MESH = pl.DeviceIdType.MESH
F32, BF16 = jnp.float32, jnp.bfloat16
WINDOWS = (2, 4, 8, 16)
RMS_EPS = 1e-06
ROUTED_SCALE = 2.5
NZ, NY, NC = 8, 4, 2
COLS = 2
PARTS = 4
TILE = 256


def rms_norm(values, gain_row):
    upcast = values.astype(F32)
    scaled = upcast * lax.rsqrt(jnp.mean(upcast * upcast, axis=-1, keepdims=True) + RMS_EPS)
    return (scaled * gain_row).astype(BF16)


def dot(a, b):
    return jnp.dot(a, b, preferred_element_type=F32)


def fused_kernel(
    dims,
    x_ref,
    gain_ref,
    ids_ref,
    score_ref,
    rep_ref,
    rept_ref,
    tgt_ref,
    tgtt_ref,
    mix_gain_ref,
    scale_ref,
    mix_ref,
    pool_ref,
    gate_ref,
    up_ref,
    down_ref,
    sgate_ref,
    sup_ref,
    sdown_ref,
    mix_out,
    moe_out,
    hbuf,
    metab,
    pick,
    back,
    wgu,
    wd,
    sendbuf,
    recv,
    xrecv,
    gu,
    hidb,
    xback,
    ret,
    rs_recv,
    shared,
    sg,
    su,
    sd,
    mixb,
    halo,
    pool,
    diff,
    mixed,
    m_sem,
    z_sem,
    ys_sem,
    yr_sem,
    x_sem,
    p_sem,
    r_sem,
    rs_sem,
    wl_sem,
    w_sem,
    wd_sem,
    sx_sem,
    sy_sem,
    sz_sem,
    sc_sem,
    mix_sem,
    halo_sem,
):
    nz, ny, nx, tok, cap, width = dims
    ring = nz // 2
    peers = ny * NC
    group = nz * cap
    half_rows = peers * group
    piece = width // COLS
    part_width = width // PARTS
    per_col = PARTS // COLS
    half = tok // 2
    ep = lax.axis_index("ep")
    tp = lax.axis_index("tp")
    z, q = ep // peers, ep % peers
    y, core = q // NC, q % NC

    def at_z(step):
        return {"ep": ((z + step + nz) % nz) * peers + q}

    def peer_of(dy, dc):
        return ((y + dy + ny) % ny) * NC + (core + dc + NC) % NC

    def at_peer(dy, dc):
        return {"ep": z * peers + peer_of(dy, dc)}

    def at_line(step):
        count = lax.axis_size("ep") * nx
        line = (ep * nx + tp + step + count) % count
        return {"ep": line // nx, "tp": line % nx}

    near = tp + 1 - 2 * (tp % 2)
    far = nx - 1 - tp
    weight_side = ({"tp": near}, {"tp": far})
    token_side = ({"tp": far}, {"tp": near})

    barrier = pltpu.get_barrier_semaphore()
    greet = [at_z(1), at_z(-1), {"tp": near}, {"tp": far}, {"tp": (tp + 2) % nx}, at_line(1), at_line(-1)]
    greet += [at_peer(r // NC, r % NC) for r in range(1, peers)]
    for device in greet:
        pl.semaphore_signal(barrier, inc=1, device_id=device, device_id_type=MESH)
    with jax.named_scope("barrier"):
        pl.semaphore_wait(barrier, len(greet))

    def remote(src, dst, send, recv_, device):
        return pltpu.make_async_remote_copy(
            src_ref=src, dst_ref=dst, send_sem=send, recv_sem=recv_, device_id=device, device_id_type=MESH
        )

    def wait_bytes(ref, sem):
        pltpu.make_async_copy(ref, ref, sem).wait()

    def wide_copies(j):
        return [
            remote(src.at[j], wgu.at[j, 2 + i], w_sem.at[0, j, i], w_sem.at[1, j, i], weight_side[j])
            for i, src in enumerate((gate_ref, up_ref))
        ]

    def down_copy(j, p):
        cols = pl.ds(p * part_width, part_width)
        return remote(
            down_ref.at[j, :, cols], wd.at[j, 1, :, cols], wd_sem.at[0, j, p], wd_sem.at[1, j, p], weight_side[j]
        )

    def own_copies(j):
        return [
            pltpu.make_async_copy(gate_ref.at[j], wgu.at[j, 0], wl_sem.at[j, 0]),
            pltpu.make_async_copy(up_ref.at[j], wgu.at[j, 1], wl_sem.at[j, 1]),
            pltpu.make_async_copy(down_ref.at[j], wd.at[j, 0], wl_sem.at[j, 2]),
        ]

    for j in range(2):
        for copy in wide_copies(j):
            copy.start()

    hold = rms_norm(x_ref[...], gain_ref[...])
    for g in range(COLS):
        hbuf[g, 0:tok] = hold[:, g * piece : (g + 1) * piece]

    def meta_copy(d, s):
        src = (-s if d == 0 else s) % nz
        dst = (-s - 1 if d == 0 else s + 1) % nz
        return remote(metab.at[src], metab.at[dst], m_sem.at[0, d, s], m_sem.at[1, d, s], at_z(1 - 2 * d))

    def z_copy(g, d, s, h):
        src = (-s if d == 0 else s) % nz
        dst = (-s - 1 if d == 0 else s + 1) % nz
        return remote(
            hbuf.at[g, pl.ds(src * tok + h * half, half)],
            hbuf.at[g, pl.ds(dst * tok + h * half, half)],
            z_sem.at[0, g, d, s, h],
            z_sem.at[1, g, d, s, h],
            at_z(1 - 2 * d),
        )

    def sends_half(d, s, h):
        return s < ring - 1 or h == d

    def meta_goes(d, s):
        return s < ring - 1 or d == 0

    def z_first(g):
        for h in range(2):
            for d in range(2):
                z_copy(g, d, 0, h).start()

    def z_forward(g, s):
        for h in range(2):
            for d in range(2):
                z_copy(g, d, s - 1, h).wait_recv()
                if sends_half(d, s, h):
                    z_copy(g, d, s, h).start()

    def last_z(g):
        for d in range(2):
            z_copy(g, d, ring - 1, d).wait_recv()

    z_first(0)
    my_ids = ids_ref[pl.ds(pl.multiple_of(tp * tok, tok), tok)].astype(F32)
    scores = score_ref[...]
    route = scores / jnp.sum(scores, axis=1, keepdims=True) * ROUTED_SCALE
    tagged = jnp.concatenate([my_ids, route, jnp.zeros((tok, tok - 8), F32)], axis=1)
    metab[0] = jnp.transpose(tagged)[:16].astype(BF16)
    for d in range(2):
        meta_copy(d, 0).start()

    for j in range(2):
        for copy in own_copies(j):
            copy.start()
    pieces = ((sgate_ref, sg, sg.shape[1] // peers), (sup_ref, su, su.shape[1] // peers), (sdown_ref, sd, sd.shape[1] // peers))
    shared_own = [pltpu.make_async_copy(src, dst.at[0], sc_sem.at[0, a]) for a, (src, dst, _) in enumerate(pieces)]
    mix_copies = [
        pltpu.make_async_copy(mix_ref, mixb, mix_sem.at[0]),
        pltpu.make_async_copy(pool_ref, pool, mix_sem.at[1]),
    ]
    reach = halo.shape[0]
    halo_copy = remote(
        mix_ref.at[pl.ds(mix_ref.shape[0] - reach, reach)], halo, halo_sem.at[0], halo_sem.at[1], at_line(1)
    )
    for copy in shared_own + mix_copies + [halo_copy]:
        copy.start()

    def piece_at(dst, size, which):
        return dst.at[pl.ds(1, nx - 1), pl.ds(which * size, size)]

    def shared_x(a, step):
        src, dst, size = pieces[a]
        rows_at = pl.ds(q * size, size)
        return remote(
            src.at[rows_at], dst.at[nx - step, rows_at], sx_sem.at[0, a], sx_sem.at[1, a], {"tp": (tp + step) % nx}
        )

    def shared_x_wait(a, side):
        _, dst, size = pieces[a]
        wait_bytes(dst.at[pl.ds(1, nx - 1), pl.ds(0, size)], sx_sem.at[side, a])

    def shared_y(a, d):
        _, dst, size = pieces[a]
        ref = piece_at(dst, size, q)
        return remote(ref, ref, sy_sem.at[0, a, d], sy_sem.at[1, a, d], at_peer(1 - 2 * d, 0))

    def shared_y2(a):
        d = a % 2
        _, dst, size = pieces[a]
        ref = piece_at(dst, size, peer_of(2 * d - 1, 0))
        return remote(ref, ref, sz_sem.at[0, a], sz_sem.at[1, a], at_peer(1 - 2 * d, 0))

    def shared_core(a, dy):
        _, dst, size = pieces[a]
        ref = piece_at(dst, size, peer_of(dy, 0))
        return remote(ref, ref, sc_sem.at[1, a], sc_sem.at[2, a], at_peer(0, 1))

    def shared_core_wait(a, side):
        _, dst, size = pieces[a]
        wait_bytes(dst.at[pl.ds(1, nx - 1), pl.ds(0, ny * size)], sc_sem.at[1 + side, a])

    for a in range(3):
        for step in (1, nx - 1, 2):
            shared_x(a, step).start()

    before = lax.broadcasted_iota(jnp.int32, (tok, tok), 0) < lax.broadcasted_iota(jnp.int32, (tok, tok), 1)
    upper = before.astype(F32).astype(BF16)
    line = lax.broadcasted_iota(jnp.int32, (2 * peers, tok), 0)
    their_core = (core + line % NC) % NC
    their_y = (y + (line % peers) // NC) % ny
    names = (2 * (z * peers + their_y * NC + their_core) + line // peers).astype(F32)

    def tables(zi):
        block = metab[zi].astype(F32)
        named = jnp.zeros((2 * peers, tok), F32)
        weight = jnp.zeros((2 * peers, tok), F32)
        for k in range(4):
            same = (block[k : k + 1] == names).astype(F32)
            named = named + same
            weight = weight + same * block[4 + k : 5 + k]
        rank = dot(named.astype(BF16), upper)
        rank = jnp.where(named > 0.5, rank, -2.0)
        spread = dot(rep_ref[...], rank.astype(BF16))
        pick[:, zi * tok : (zi + 1) * tok] = (spread == tgt_ref[:, zi : zi + 1]).astype(F32).astype(BF16)
        padding = jnp.zeros((tok - 4 * peers, tok), F32)
        turned = jnp.transpose(jnp.concatenate([rank, weight, padding], axis=0))
        spread_t = dot(turned[:, : 2 * peers].astype(BF16), rept_ref[...])
        weight_t = dot(turned[:, 2 * peers : 4 * peers].astype(BF16), rept_ref[...])
        back[zi] = jnp.where(spread_t == tgtt_ref[zi : zi + 1], weight_t, 0.0).astype(BF16)

    def select(g):
        def body(n, _):
            cols = pl.ds(pl.multiple_of(n * TILE, TILE), TILE)
            sendbuf[g, :, cols] = dot(pick[...], hbuf[g, :, cols]).astype(BF16)
            return 0

        lax.fori_loop(0, piece // TILE, body, 0)
        for j in range(2):
            recv[g, j * half_rows : j * half_rows + group] = sendbuf[g, j * half_rows : j * half_rows + group]

    def y_copy(g, j, r):
        part = pl.ds(j * half_rows + r * group, group)
        return remote(
            sendbuf.at[g, part], recv.at[g, part], ys_sem.at[g], yr_sem.at[g, j, r], at_peer(r // NC, r % NC)
        )

    def x_copy(g, j, r):
        part = pl.ds(j * half_rows + r * group, group)
        return remote(recv.at[g, part], xrecv.at[g, part], x_sem.at[0, g, j], x_sem.at[1, g, j], token_side[j])

    order = list(range(1, peers))
    order.sort(key=lambda r: min(r // NC, ny - r // NC))

    def y_start(g):
        for r in order[::-1]:
            for j in range(2):
                y_copy(g, j, r).start()
        for j in range(2):
            x_copy(g, j, 0).start()

    def x_forward(g, some):
        for r in some:
            for j in range(2):
                y_copy(g, j, r).wait_recv()
                x_copy(g, j, r).start()

    def gate_up(which, g, j):
        src = (recv, xrecv)[which]

        def body(n, _):
            part = dot(src[g, j * half_rows : (j + 1) * half_rows], wgu[j, n, g * piece : (g + 1) * piece])
            if g == 0:
                gu[which, j, n] = part
            else:
                gu[which, j, n] = gu[which, j, n] + part
            return 0

        lax.fori_loop(0, 4, body, 0)

    def hidden(which, j):
        for i in range(2):
            gate = gu[which, j, i * 2]
            hidb[which, j, i] = (gate / (1.0 + jnp.exp(-gate)) * gu[which, j, i * 2 + 1]).astype(BF16)

    def down(which, p, j, dst):
        g = p // per_col

        def body(n, _):
            cols = pl.ds(pl.multiple_of((p % per_col) * part_width + n * TILE, TILE), TILE)
            wide = pl.ds(pl.multiple_of(p * part_width + n * TILE, TILE), TILE)
            val = dot(hidb[which, j, 0], wd[j, 0, :, wide]) + dot(hidb[which, j, 1], wd[j, 1, :, wide])
            dst[g, j * half_rows : (j + 1) * half_rows, cols] = val.astype(BF16)
            return 0

        lax.fori_loop(0, part_width // TILE, body, 0)

    def at_part(ref, p, rows_at):
        return ref.at[p // per_col, rows_at, pl.ds((p % per_col) * part_width, part_width)]

    def p_copy(p, j):
        rows_at = pl.ds(j * half_rows, half_rows)
        return remote(
            at_part(sendbuf, p, rows_at), at_part(xback, p, rows_at), p_sem.at[0, p, j], p_sem.at[1, p, j], token_side[j]
        )

    def r_copy(p, j, r):
        rows_at = pl.ds(j * half_rows + r * group, group)
        return remote(
            at_part(recv, p, rows_at),
            at_part(ret, p, rows_at),
            r_sem.at[0, p],
            r_sem.at[1, p],
            at_peer(-(r // NC), -(r % NC)),
        )

    def mixer():
        for copy in mix_copies:
            copy.wait()
        halo_copy.wait_recv()
        count = mixb.shape[0]
        lead = jnp.where(ep * nx + tp > 0, 1.0, 0.0)
        body_in = mixb[...].astype(F32)
        halo_in = halo[...].astype(F32) * lead
        scales = [
            lax.rsqrt(jnp.mean(v * v, axis=-1, keepdims=True) + RMS_EPS) for v in (halo_in, body_in)
        ]
        position = (ep * nx + tp) * count + lax.broadcasted_iota(jnp.int32, (count, 1), 0)
        span_width = width // len(WINDOWS)
        for g, span in enumerate(WINDOWS):
            counts = jnp.minimum(position + 1, span).astype(F32)
            for n in range(span_width // TILE):
                cols = slice(g * span_width + n * TILE, g * span_width + (n + 1) * TILE)
                gain = mix_gain_ref[:, cols]
                top = (halo[:, cols].astype(F32) * lead * scales[0] * gain).astype(BF16).astype(F32)
                rest = (mixb[:, cols].astype(F32) * scales[1] * gain).astype(BF16).astype(F32)
                total = jnp.concatenate([top, rest], axis=0)
                step = 1
                while step < span:
                    total = total + pltpu.roll(total, step, 0)
                    step *= 2
                diff[:, n * TILE : (n + 1) * TILE] = (total[reach:] / counts - rest).astype(BF16)
            cols = slice(g * span_width, (g + 1) * span_width)
            mixed[:, cols] = (dot(diff[...], pool[g]) * scale_ref[:, cols]).astype(BF16)
        pltpu.make_async_copy(mixed, mix_out, mix_sem.at[2]).start()

    def shared_expert():
        for a in range(3):
            shared_own[a].wait()
            shared_core_wait(a, 1)
        again = rms_norm(x_ref[...], gain_ref[...])
        tokens = [again[:, g * piece : (g + 1) * piece] for g in range(COLS)]
        hids = []
        for i in range(nx):
            gate = dot(tokens[0], sg[i, :piece]) + dot(tokens[1], sg[i, piece:])
            up = dot(tokens[0], su[i, :piece]) + dot(tokens[1], su[i, piece:])
            hids.append((gate / (1.0 + jnp.exp(-gate)) * up).astype(BF16))

        def body(n, _):
            cols = pl.ds(pl.multiple_of(n * TILE, TILE), TILE)
            total = dot(hids[0], sd[0, :, cols])
            for i in range(1, nx):
                total = total + dot(hids[i], sd[i, :, cols])
            shared[:, cols] = total
            return 0

        lax.fori_loop(0, width // TILE, body, 0)

    def rs_at(ref, p, d, s, first, count):
        return ref.at[
            p // per_col,
            pl.ds((d * ring + s) * tok + first, count),
            pl.ds((p % per_col) * part_width, part_width),
        ]

    def rs_copy(p, d, s):
        first, count = (d * half, half) if s == 0 else (0, tok)
        return remote(
            rs_at(hbuf, p, d, s, first, count),
            rs_at(rs_recv, p, d, s, first, count),
            rs_sem.at[0, p, d, s],
            rs_sem.at[1, p, d, s],
            at_z(1 - 2 * d),
        )

    def share(p, zi, first, count, adds, place):
        g = p // per_col

        def body(n, _):
            cols = pl.ds(pl.multiple_of((p % per_col) * part_width + n * TILE, TILE), TILE)
            total = dot(back[zi, first : first + count], ret[g, :, cols])
            for d, s in adds:
                at = (d * ring + s) * tok + first
                total = total + rs_recv[g, at : at + count, cols].astype(F32)
            if place is None:
                wide = pl.ds(pl.multiple_of(p * part_width + n * TILE, TILE), TILE)
                moe_out[first : first + count, wide] = (total + shared[first : first + count, wide]).astype(BF16)
            else:
                hbuf[g, place + first : place + first + count, cols] = total.astype(BF16)
            return 0

        lax.fori_loop(0, part_width // TILE, body, 0)

    def rs_step(p, s):
        for d in range(2):
            zi = ring - s if d == 0 else ring + s
            place = (d * ring + s) * tok
            if s > 0:
                with jax.named_scope(f"rswait{p}_{s}"):
                    rs_copy(p, d, s - 1).wait_recv()
            if s == 0:
                share(p, zi, d * half, half, (), place)
            elif s == 1:
                for h in range(2):
                    share(p, zi, h * half, half, ((d, 0),) if h == d else (), place)
            else:
                share(p, zi, 0, tok, ((d, s - 1),), place)
            rs_copy(p, d, s).start()

    def rs_last(p):
        with jax.named_scope(f"rswait{p}_last"):
            for d in range(2):
                rs_copy(p, d, ring - 1).wait_recv()
        share(p, 0, 0, tok, ((0, ring - 1), (1, ring - 1)), None)

    def ret_wait(p):
        with jax.named_scope(f"retwait{p}"):
            far_rows = 2 * (half_rows - group)
            wait_bytes(at_part(ret, p, pl.ds(0, far_rows)), r_sem.at[1, p])

    def give_back(p):
        cols = slice((p % per_col) * part_width, (p % per_col + 1) * part_width)
        g = p // per_col
        for j in range(2):
            with jax.named_scope(f"pwait{p}{j}"):
                p_copy(p, j).wait_recv()
            span = slice(j * half_rows, (j + 1) * half_rows)
            recv[g, span, cols] = (recv[g, span, cols].astype(F32) + xback[g, span, cols].astype(F32)).astype(BF16)
            for r in order[::-1]:
                r_copy(p, j, r).start()
            first = slice(j * half_rows, j * half_rows + group)
            ret[g, first, cols] = recv[g, first, cols]

    for s in range(1, ring):
        with jax.named_scope(f"z0_{s}"):
            for d in range(2):
                meta_copy(d, s - 1).wait_recv()
                if meta_goes(d, s):
                    meta_copy(d, s).start()
            z_forward(0, s)
    z_first(1)
    meta_copy(0, ring - 1).wait_recv()
    with jax.named_scope("tables"):
        for zi in range(nz):
            tables(zi)
    with jax.named_scope("last_z0"):
        last_z(0)
    with jax.named_scope("select0"):
        select(0)
        y_start(0)
    for s in range(1, ring):
        with jax.named_scope(f"z1_{s}"):
            z_forward(1, s)
        with jax.named_scope(f"xfwd0_{s}"):
            x_forward(0, order[(s - 1) * len(order) // ring : s * len(order) // ring])
        for j in range(2):
            down_copy(j, s - 1).start()
    with jax.named_scope("xfwd0_rest"):
        x_forward(0, order[(ring - 1) * len(order) // ring :])
    with jax.named_scope("last_z1"):
        last_z(1)
    with jax.named_scope("select1"):
        select(1)
        y_start(1)
    for j in range(2):
        for p in range(ring - 1, PARTS):
            down_copy(j, p).start()
    with jax.named_scope("weights"):
        for j in range(2):
            for copy in own_copies(j):
                copy.wait()
            for copy in wide_copies(j):
                copy.wait_recv()
    with jax.named_scope("own_gu0"):
        for j in range(2):
            gate_up(0, 0, j)
    with jax.named_scope("xfwd1"):
        x_forward(1, order)
    with jax.named_scope("shared_x"):
        for a in range(3):
            shared_x_wait(a, 1)
            for d in range(2):
                shared_y(a, d).start()
    with jax.named_scope("mixer"):
        mixer()
    with jax.named_scope("shared_y"):
        for a in range(3):
            for d in range(2):
                shared_y(a, d).wait_recv()
            shared_y2(a).start()
            for dy in (0, 1, -1):
                shared_core(a, dy).start()
    for j in range(2):
        with jax.named_scope(f"xwait0_{j}"):
            wait_bytes(xrecv.at[0, pl.ds(j * half_rows, half_rows)], x_sem.at[1, 0, j])
        with jax.named_scope("par_gu0"):
            gate_up(1, 0, j)
    with jax.named_scope("own_gu1"):
        for j in range(2):
            gate_up(0, 1, j)
            hidden(0, j)
    far_rows = 2 * (half_rows - group)
    for g in range(COLS):
        wait_bytes(sendbuf.at[g, pl.ds(0, far_rows)], ys_sem.at[g])
    for j in range(2):
        with jax.named_scope(f"xwait1_{j}"):
            wait_bytes(xrecv.at[1, pl.ds(j * half_rows, half_rows)], x_sem.at[1, 1, j])
        with jax.named_scope("par_gu1"):
            gate_up(1, 1, j)
            hidden(1, j)
    for p in range(PARTS):
        for j in range(2):
            with jax.named_scope(f"wd{p}{j}"):
                down_copy(j, p).wait_recv()
            with jax.named_scope("par_down"):
                down(1, p, j, sendbuf)
                p_copy(p, j).start()
    for g in range(COLS):
        for j in range(2):
            wait_bytes(recv.at[g, pl.ds(0, half_rows)], x_sem.at[0, g, j])
    with jax.named_scope("own_down"):
        for p in range(PARTS):
            for j in range(2):
                down(0, p, j, recv)
    for g in range(COLS):
        for d in range(2):
            for s in range(ring):
                for h in range(2):
                    if sends_half(d, s, h):
                        z_copy(g, d, s, h).wait_send()
    with jax.named_scope("shared"):
        for a in range(3):
            shared_y2(a).wait_recv()
            shared_core(a, 2).start()
        shared_expert()

    events = []
    for p in range(PARTS):
        events.append((9 * p, give_back, (p,)))
        events.append((9 * p + 11, ret_wait, (p,)))
        for s in range(ring):
            events.append((9 * p + 12 + 5 * s, rs_step, (p, s)))
        events.append((9 * p + 12 + 5 * ring, rs_last, (p,)))
    for _, act, args in sorted(events, key=lambda e: e[0]):
        act(*args)

    pltpu.make_async_copy(mixed, mix_out, mix_sem.at[2]).wait()
    halo_copy.wait_send()
    for d in range(2):
        for s in range(ring):
            if meta_goes(d, s):
                meta_copy(d, s).wait_send()
    for p in range(PARTS):
        wait_bytes(at_part(ret, p, pl.ds(0, far_rows)), r_sem.at[0, p])
        for d in range(2):
            for s in range(ring):
                rs_copy(p, d, s).wait_send()
        for j in range(2):
            p_copy(p, j).wait_send()
            down_copy(j, p).wait_send()
    for j in range(2):
        for copy in wide_copies(j):
            copy.wait_send()
    for a in range(3):
        shared_x_wait(a, 0)
        shared_y2(a).wait_send()
        shared_core_wait(a, 0)
        for d in range(2):
            shared_y(a, d).wait_send()


def fused(dims, moe_input, moe_gain, ids, scores, mix_gain, scale, mix_input, pool, routed, shared):
    nz, ny, nx, tok, cap, width = dims
    peers, ring = ny * NC, nz // 2
    group = nz * cap
    half_rows = peers * group
    rows = 2 * half_rows
    piece = width // COLS
    hid = routed[0].shape[2]
    sh = shared[0].shape[1]
    count = mix_input.shape[0]
    line = np.arange(rows)
    rep = (line[:, None] // group == np.arange(2 * peers)[None, :]).astype(np.float32)
    turn = (line // cap) % nz
    tgt = np.where(turn[:, None] == np.arange(nz)[None, :], (line % cap)[:, None], -1).astype(np.float32)
    vmem = pl.BlockSpec(memory_space=pltpu.VMEM)
    hbm = pl.BlockSpec(memory_space=pl.ANY)
    dma = pltpu.SemaphoreType.DMA
    return pl.pallas_call(
        functools.partial(fused_kernel, dims),
        out_shape=(jax.ShapeDtypeStruct((count, width), BF16), jax.ShapeDtypeStruct((tok, width), BF16)),
        in_specs=[vmem] * 10 + [hbm] * 8,
        out_specs=(hbm, vmem),
        scratch_shapes=[
            pltpu.VMEM((COLS, nz * tok, piece), BF16),
            pltpu.VMEM((nz, 16, tok), BF16),
            pltpu.VMEM((rows, nz * tok), BF16),
            pltpu.VMEM((nz, tok, rows), BF16),
            pltpu.VMEM((2, 4, width, hid), BF16),
            pltpu.VMEM((2, 2, hid, width), BF16),
            pltpu.VMEM((COLS, rows, piece), BF16),
            pltpu.VMEM((COLS, rows, piece), BF16),
            pltpu.VMEM((COLS, rows, piece), BF16),
            pltpu.VMEM((2, 2, 4, half_rows, hid), F32),
            pltpu.VMEM((2, 2, 2, half_rows, hid), BF16),
            pltpu.VMEM((COLS, rows, piece), BF16),
            pltpu.VMEM((COLS, rows, piece), BF16),
            pltpu.VMEM((COLS, nz * tok, piece), BF16),
            pltpu.VMEM((tok, width), F32),
            pltpu.VMEM((nx, width, sh), BF16),
            pltpu.VMEM((nx, width, sh), BF16),
            pltpu.VMEM((nx, sh, width), BF16),
            pltpu.VMEM((count, width), BF16),
            pltpu.VMEM((16, width), BF16),
            pltpu.VMEM(pool.shape, BF16),
            pltpu.VMEM((count, width // len(WINDOWS)), BF16),
            pltpu.VMEM((count, width), BF16),
            dma((2, 2, ring)),
            dma((2, COLS, 2, ring, 2)),
            dma((COLS,)),
            dma((COLS, 2, peers)),
            dma((2, COLS, 2)),
            dma((2, PARTS, 2)),
            dma((2, PARTS)),
            dma((2, PARTS, 2, ring)),
            dma((2, 3)),
            dma((2, 2, 2)),
            dma((2, 2, PARTS)),
            dma((2, 3)),
            dma((2, 3, 2)),
            dma((2, 3)),
            dma((3, 3)),
            dma((3,)),
            dma((2,)),
        ],
        compiler_params=pltpu.CompilerParams(
            collective_id=0, has_side_effects=True, vmem_limit_bytes=67043328
        ),
    )(
        moe_input,
        moe_gain.reshape(1, width),
        ids,
        scores,
        jnp.asarray(rep, BF16),
        jnp.asarray(rep.T, BF16),
        jnp.asarray(tgt),
        jnp.asarray(tgt.T),
        mix_gain.reshape(1, width),
        scale.reshape(1, width),
        mix_input,
        pool,
        *routed,
        *shared,
    )


def per_device(
    sizes,
    mix_input,
    mix_gain,
    pool_weight,
    pool_scale,
    moe_input,
    moe_gain,
    expert_ids,
    route_score,
    expert_gate,
    expert_up,
    expert_down,
    shared_gate,
    shared_up,
    shared_down,
):
    nz, ny = sizes
    tok, width = moe_input.shape
    experts = lax.axis_size("ep") * expert_gate.shape[0]
    cap = 3 * tok * expert_ids.shape[1] // (2 * experts)
    dims = (nz, ny, lax.axis_size("tp"), tok, cap, width)
    return fused(
        dims,
        moe_input,
        moe_gain,
        expert_ids,
        route_score,
        mix_gain,
        pool_scale,
        mix_input,
        pool_weight,
        (expert_gate, expert_up, expert_down),
        (shared_gate, shared_up, shared_down),
    )


def solution(mesh, sizes=(NZ, NY)):
    return jax.shard_map(
        functools.partial(per_device, sizes),
        mesh=mesh,
        in_specs=(
            P(("ep", "tp"), None),
            P(),
            P(),
            P(),
            P(("ep", "tp"), None),
            P(),
            P("ep", None),
            P(("ep", "tp"), None),
            P("ep", None, "tp"),
            P("ep", None, "tp"),
            P("ep", "tp", None),
            P(None, "tp"),
            P(None, "tp"),
            P("tp", None),
        ),
        out_specs=(P(("ep", "tp"), None), P(("ep", "tp"), None)),
        check_vma=False,
    )
```

```python
import functools

import jax
import jax.numpy as jnp
import numpy as np
from jax import lax
from jax.experimental import pallas as pl
from jax.experimental.pallas import tpu as pltpu
from jax.sharding import PartitionSpec as P

MESH = pl.DeviceIdType.MESH
F32, BF16 = jnp.float32, jnp.bfloat16
WINDOWS = (2, 4, 8, 16)
RMS_EPS = 1e-06
ROUTED_SCALE = 2.5
NZ, NY, NC = 8, 4, 2
COLS = 2
WIDTHS = (256, 256, 256, 256, 256, 256, 256, 128, 128)
PARTS = len(WIDTHS)
TILE = 256
GAP, HOP, LEAD, GIVE, AHEAD = 7.0, 5.5, 3.0, 1.0, 2
SHARED_AT = (6.5, 16.2, 27.5)


def rms_norm(values, gain_row):
    upcast = values.astype(F32)
    scaled = upcast * lax.rsqrt(jnp.mean(upcast * upcast, axis=-1, keepdims=True) + RMS_EPS)
    return (scaled * gain_row).astype(BF16)


def dot(a, b):
    return jnp.dot(a, b, preferred_element_type=F32)


def fused_kernel(
    dims,
    x_hbm,
    gain_ref,
    ids_ref,
    score_ref,
    rep_hbm,
    rept_hbm,
    tgt_hbm,
    tgtt_hbm,
    mix_gain_ref,
    scale_ref,
    mix_ref,
    pool_ref,
    gate_ref,
    up_ref,
    down_ref,
    sgate_ref,
    sup_ref,
    sdown_ref,
    mix_out,
    moe_out,
    hbuf,
    metab,
    pick,
    back,
    wgu,
    wd,
    sendbuf,
    recv,
    xrecv,
    gu,
    hidb,
    own,
    xback,
    ret,
    rs_recv,
    shared,
    sg,
    su,
    sd,
    mixb,
    halo,
    pool,
    x_ref,
    rep_ref,
    rept_ref,
    tgt_ref,
    tgtt_ref,
    diff,
    mixed,
    m_sem,
    z_sem,
    ys_sem,
    yr_sem,
    x_sem,
    p_sem,
    r_sem,
    rs_sem,
    wl_sem,
    w_sem,
    wd_sem,
    sx_sem,
    sy_sem,
    sz_sem,
    sr_sem,
    sc_sem,
    mix_sem,
    halo_sem,
    in_sem,
):
    nz, ny, nx, tok, cap, width = dims
    ring = nz // 2
    peers = ny * NC
    group = nz * cap
    half_rows = peers * group
    piece = width // COLS
    scale = width // sum(WIDTHS)
    starts = [sum(WIDTHS[:p]) * scale for p in range(PARTS)]
    widths = [w * scale for w in WIDTHS]

    def col_of(p):
        return starts[p] // piece

    def cols_of(p):
        return slice(starts[p] % piece, starts[p] % piece + widths[p])

    def span_of(p):
        return pl.ds(starts[p] % piece, widths[p])
    half = tok // 2
    ep = lax.axis_index("ep")
    tp = lax.axis_index("tp")
    z, q = ep // peers, ep % peers
    y, core = q // NC, q % NC

    def at_z(step):
        return {"ep": ((z + step + nz) % nz) * peers + q}

    def peer_of(dy, dc):
        return ((y + dy + ny) % ny) * NC + (core + dc + NC) % NC

    def at_peer(dy, dc):
        return {"ep": z * peers + peer_of(dy, dc)}

    def at_line(step):
        count = lax.axis_size("ep") * nx
        line = (ep * nx + tp + step + count) % count
        return {"ep": line // nx, "tp": line % nx}

    near = tp + 1 - 2 * (tp % 2)
    far = nx - 1 - tp
    weight_side = ({"tp": near}, {"tp": far})
    token_side = ({"tp": far}, {"tp": near})

    loads = [
        pltpu.make_async_copy(src, dst, in_sem.at[i])
        for i, (src, dst) in enumerate(
            ((x_hbm, x_ref), (rep_hbm, rep_ref), (rept_hbm, rept_ref), (tgt_hbm, tgt_ref), (tgtt_hbm, tgtt_ref))
        )
    ]
    for copy in loads:
        copy.start()

    barrier = pltpu.get_barrier_semaphore()
    greet = [at_z(step) for step in range(1, nz)] + [{"tp": near}, {"tp": far}, {"tp": (tp + 2) % nx}, at_line(1), at_line(-1)]
    greet += [at_peer(r // NC, r % NC) for r in range(1, peers)]
    for device in greet:
        pl.semaphore_signal(barrier, inc=1, device_id=device, device_id_type=MESH)
    with jax.named_scope("barrier"):
        pl.semaphore_wait(barrier, len(greet))

    def remote(src, dst, send, recv_, device):
        return pltpu.make_async_remote_copy(
            src_ref=src, dst_ref=dst, send_sem=send, recv_sem=recv_, device_id=device, device_id_type=MESH
        )

    def wait_bytes(ref, sem):
        pltpu.make_async_copy(ref, ref, sem).wait()

    def wide_copies(j):
        return [
            remote(src.at[j], wgu.at[j, 2 + i], w_sem.at[0, j, i], w_sem.at[1, j, i], weight_side[j])
            for i, src in enumerate((gate_ref, up_ref))
        ]

    def down_copy(j, p):
        cols = pl.ds(starts[p], widths[p])
        return remote(
            down_ref.at[j, :, cols], wd.at[j, 1, :, cols], wd_sem.at[0, j, p], wd_sem.at[1, j, p], weight_side[j]
        )

    def own_copies(j):
        return [
            pltpu.make_async_copy(gate_ref.at[j], wgu.at[j, 0], wl_sem.at[j, 0]),
            pltpu.make_async_copy(up_ref.at[j], wgu.at[j, 1], wl_sem.at[j, 1]),
            pltpu.make_async_copy(down_ref.at[j], wd.at[j, 0], wl_sem.at[j, 2]),
        ]

    for j in range(2):
        for copy in wide_copies(j):
            copy.start()

    loads[0].wait()
    hold = rms_norm(x_ref[...], gain_ref[...])
    for g in range(COLS):
        hbuf[g, 0:tok] = hold[:, g * piece : (g + 1) * piece]

    def meta_copy(d, s):
        src = (-s if d == 0 else s) % nz
        dst = (-s - 1 if d == 0 else s + 1) % nz
        return remote(metab.at[src], metab.at[dst], m_sem.at[0, d, s], m_sem.at[1, d, s], at_z(1 - 2 * d))

    def z_copy(g, d, s, h):
        src = (-s if d == 0 else s) % nz
        dst = (-s - 1 if d == 0 else s + 1) % nz
        return remote(
            hbuf.at[g, pl.ds(src * tok + h * half, half)],
            hbuf.at[g, pl.ds(dst * tok + h * half, half)],
            z_sem.at[0, g, d, s, h],
            z_sem.at[1, g, d, s, h],
            at_z(1 - 2 * d),
        )

    def sends_half(d, s, h):
        return s < ring - 1 or h == d

    def meta_goes(d, s):
        return s < ring - 1 or d == 0

    def z_first(g):
        for h in range(2):
            for d in range(2):
                z_copy(g, d, 0, h).start()

    def z_forward(g, s):
        for h in range(2):
            for d in range(2):
                z_copy(g, d, s - 1, h).wait_recv()
                if sends_half(d, s, h):
                    z_copy(g, d, s, h).start()

    def last_z(g):
        for d in range(2):
            z_copy(g, d, ring - 1, d).wait_recv()

    z_first(0)
    my_ids = ids_ref[:, pl.ds(pl.multiple_of(tp * tok, tok), tok)].astype(F32)
    scores = score_ref[...]
    route = scores / jnp.sum(scores, axis=0, keepdims=True) * ROUTED_SCALE
    metab[0] = jnp.concatenate([my_ids, route, jnp.zeros((8, tok), F32)], axis=0).astype(BF16)
    for d in range(2):
        meta_copy(d, 0).start()

    for j in range(2):
        for copy in own_copies(j):
            copy.start()
    pieces = ((sgate_ref, sg, sg.shape[1] // peers), (sup_ref, su, su.shape[1] // peers), (sdown_ref, sd, sd.shape[1] // peers))
    shared_own = [pltpu.make_async_copy(src, dst.at[0], sc_sem.at[0, a]) for a, (src, dst, _) in enumerate(pieces)]
    mix_copies = [
        pltpu.make_async_copy(mix_ref, mixb, mix_sem.at[0]),
        pltpu.make_async_copy(pool_ref, pool, mix_sem.at[1]),
    ]
    reach = halo.shape[0]
    halo_copy = remote(
        mix_ref.at[pl.ds(mix_ref.shape[0] - reach, reach)], halo, halo_sem.at[0], halo_sem.at[1], at_line(1)
    )
    for copy in shared_own + mix_copies + [halo_copy]:
        copy.start()

    def piece_at(dst, size, which):
        return dst.at[pl.ds(1, nx - 1), pl.ds(which * size, size)]

    def crumb(a):
        _, dst, size = pieces[a]
        if a < 2:
            small = size // nz
            return (pl.ds(q * size + z * small, small),)
        small = dst.shape[2] // nz
        return (pl.ds(q * size, size), pl.ds(pl.multiple_of(z * small, small), small))

    def crumbs(a, count):
        _, dst, size = pieces[a]
        if a < 2:
            return dst.at[pl.ds(1, nx - 1), pl.ds(0, count * (size // nz))]
        return dst.at[pl.ds(1, nx - 1), pl.ds(0, size), pl.ds(0, count * (dst.shape[2] // nz))]

    def shared_x(a, step):
        src, dst, _ = pieces[a]
        at = crumb(a)
        return remote(
            src.at[at], dst.at[(nx - step, *at)], sx_sem.at[0, a], sx_sem.at[1, a], {"tp": (tp + step) % nx}
        )

    def shared_x_wait(a, side):
        wait_bytes(crumbs(a, 1), sx_sem.at[side, a])

    def shared_z(a, step):
        _, dst, _ = pieces[a]
        ref = dst.at[(pl.ds(1, nx - 1), *crumb(a))]
        return remote(ref, ref, sr_sem.at[0, a], sr_sem.at[1, a], at_z(step))

    def shared_z_wait(a, side):
        wait_bytes(crumbs(a, nz - 1), sr_sem.at[side, a])

    def shared_y(a, d):
        _, dst, size = pieces[a]
        ref = piece_at(dst, size, q)
        return remote(ref, ref, sy_sem.at[0, a, d], sy_sem.at[1, a, d], at_peer(1 - 2 * d, 0))

    def shared_y2(a):
        d = a % 2
        _, dst, size = pieces[a]
        ref = piece_at(dst, size, peer_of(2 * d - 1, 0))
        return remote(ref, ref, sz_sem.at[0, a], sz_sem.at[1, a], at_peer(1 - 2 * d, 0))

    def shared_core(a, dy):
        _, dst, size = pieces[a]
        ref = piece_at(dst, size, peer_of(dy, 0))
        return remote(ref, ref, sc_sem.at[1, a], sc_sem.at[2, a], at_peer(0, 1))

    def shared_core_wait(a, side):
        _, dst, size = pieces[a]
        wait_bytes(dst.at[pl.ds(1, nx - 1), pl.ds(0, ny * size)], sc_sem.at[1 + side, a])

    for a in range(3):
        for step in (1, nx - 1, 2):
            shared_x(a, step).start()

    before = lax.broadcasted_iota(jnp.int32, (tok, tok), 0) < lax.broadcasted_iota(jnp.int32, (tok, tok), 1)
    upper = before.astype(F32).astype(BF16)
    line = lax.broadcasted_iota(jnp.int32, (2 * peers, tok), 0)
    their_core = (core + line % NC) % NC
    their_y = (y + (line % peers) // NC) % ny
    names = (2 * (z * peers + their_y * NC + their_core) + line // peers).astype(F32)

    def tables(zi):
        block = metab[zi].astype(F32)
        named = jnp.zeros((2 * peers, tok), F32)
        weight = jnp.zeros((2 * peers, tok), F32)
        for k in range(4):
            same = (block[k : k + 1] == names).astype(F32)
            named = named + same
            weight = weight + same * block[4 + k : 5 + k]
        rank = dot(named.astype(BF16), upper)
        rank = jnp.where(named > 0.5, rank, -2.0)
        spread = dot(rep_ref[...], rank.astype(BF16))
        pick[:, zi * tok : (zi + 1) * tok] = (spread == tgt_ref[:, zi : zi + 1]).astype(F32).astype(BF16)
        padding = jnp.zeros((tok - 4 * peers, tok), F32)
        turned = jnp.transpose(jnp.concatenate([rank, weight, padding], axis=0))
        spread_t = dot(turned[:, : 2 * peers].astype(BF16), rept_ref[...])
        weight_t = dot(turned[:, 2 * peers : 4 * peers].astype(BF16), rept_ref[...])
        back[zi * tok : (zi + 1) * tok] = jnp.where(spread_t == tgtt_ref[zi : zi + 1], weight_t, 0.0).astype(BF16)

    def select(g):
        def body(n, _):
            cols = pl.ds(pl.multiple_of(n * TILE, TILE), TILE)
            sendbuf[g, :, cols] = dot(pick[...], hbuf[g, :, cols]).astype(BF16)
            return 0

        lax.fori_loop(0, piece // TILE, body, 0)
        for j in range(2):
            recv[g, j * half_rows : j * half_rows + group] = sendbuf[g, j * half_rows : j * half_rows + group]

    def y_copy(g, j, r):
        part = pl.ds(j * half_rows + r * group, group)
        return remote(
            sendbuf.at[g, part], recv.at[g, part], ys_sem.at[g], yr_sem.at[g, j, r], at_peer(r // NC, r % NC)
        )

    def x_copy(g, j, r):
        part = pl.ds(j * half_rows + r * group, group)
        return remote(recv.at[g, part], xrecv.at[g, part], x_sem.at[0, g, j], x_sem.at[1, g, j], token_side[j])

    order = list(range(1, peers))
    order.sort(key=lambda r: min(r // NC, ny - r // NC))

    def y_start(g):
        for r in order[::-1]:
            for j in range(2):
                y_copy(g, j, r).start()
        for j in range(2):
            x_copy(g, j, 0).start()

    def x_forward(g, some):
        for r in some:
            for j in range(2):
                y_copy(g, j, r).wait_recv()
                x_copy(g, j, r).start()

    def gate_up(which, g, j):
        src = (recv, xrecv)[which]

        def body(n, _):
            part = dot(src[g, j * half_rows : (j + 1) * half_rows], wgu[j, n, g * piece : (g + 1) * piece])
            at = pl.ds(pl.multiple_of(((which * 2 + j) * 4 + n) * half_rows, half_rows), half_rows)
            if g == 0:
                gu[at] = part
            else:
                gu[at] = gu[at] + part
            return 0

        lax.fori_loop(0, 4, body, 0)

    def hidden(which, j):
        for i in range(2):
            at = ((which * 2 + j) * 4 + i * 2) * half_rows
            gate = gu[at : at + half_rows]
            up = gu[at + half_rows : at + 2 * half_rows]
            hidb[which, j, i] = (gate / (1.0 + jnp.exp(-gate)) * up).astype(BF16)

    def down(which, p, j):
        wide = slice(starts[p], starts[p] + widths[p])
        val = dot(hidb[which, j, 0], wd[j, 0, :, wide]) + dot(hidb[which, j, 1], wd[j, 1, :, wide])
        if which == 0:
            own[col_of(p), j, :, cols_of(p)] = val.astype(BF16)
        else:
            sendbuf[col_of(p), j * half_rows : (j + 1) * half_rows, cols_of(p)] = val.astype(BF16)

    def at_part(ref, p, which, rows_at):
        return ref.at[col_of(p), which, rows_at, span_of(p)]

    def p_copy(p, j):
        return remote(
            sendbuf.at[col_of(p), pl.ds(j * half_rows, half_rows), span_of(p)],
            at_part(xback, p, j, pl.ds(0, half_rows)),
            p_sem.at[0, p, j],
            p_sem.at[1, p, j],
            token_side[j],
        )

    def r_copy(p, r):
        rows_at, both = pl.ds(r * group, group), pl.ds(0, 2)
        return remote(
            at_part(own, p, both, rows_at),
            at_part(ret, p, both, rows_at),
            r_sem.at[0, p],
            r_sem.at[1, p],
            at_peer(-(r // NC), -(r % NC)),
        )

    def r_wait(p, side):
        wait_bytes(at_part(ret, p, pl.ds(0, 2), pl.ds(0, half_rows - group)), r_sem.at[side, p])

    def mixer():
        for copy in mix_copies:
            copy.wait()
        halo_copy.wait_recv()
        count = mixb.shape[0]
        lead = jnp.where(ep * nx + tp > 0, 1.0, 0.0)
        body_in = mixb[...].astype(F32)
        halo_in = halo[...].astype(F32) * lead
        scales = [
            lax.rsqrt(jnp.mean(v * v, axis=-1, keepdims=True) + RMS_EPS) for v in (halo_in, body_in)
        ]
        position = (ep * nx + tp) * count + lax.broadcasted_iota(jnp.int32, (count, 1), 0)
        span_width = width // len(WINDOWS)
        for g, span in enumerate(WINDOWS):
            counts = jnp.minimum(position + 1, span).astype(F32)
            for n in range(span_width // TILE):
                cols = slice(g * span_width + n * TILE, g * span_width + (n + 1) * TILE)
                gain = mix_gain_ref[:, cols]
                top = (halo[:, cols].astype(F32) * lead * scales[0] * gain).astype(BF16).astype(F32)
                rest = (mixb[:, cols].astype(F32) * scales[1] * gain).astype(BF16).astype(F32)
                total = jnp.concatenate([top, rest], axis=0)
                step = 1
                while step < span:
                    total = total + pltpu.roll(total, step, 0)
                    step *= 2
                diff[:, n * TILE : (n + 1) * TILE] = (total[reach:] / counts - rest).astype(BF16)
            cols = slice(g * span_width, (g + 1) * span_width)
            mixed[:, cols] = (dot(diff[...], pool[g]) * scale_ref[:, cols]).astype(BF16)
        pltpu.make_async_copy(mixed, mix_out, mix_sem.at[2]).start()

    def shared_expert():
        for a in range(3):
            shared_own[a].wait()
            shared_core_wait(a, 1)
        again = rms_norm(x_ref[...], gain_ref[...])
        tokens = [again[:, g * piece : (g + 1) * piece] for g in range(COLS)]
        hids = []
        for i in range(nx):
            gate = dot(tokens[0], sg[i, :piece]) + dot(tokens[1], sg[i, piece:])
            up = dot(tokens[0], su[i, :piece]) + dot(tokens[1], su[i, piece:])
            hids.append((gate / (1.0 + jnp.exp(-gate)) * up).astype(BF16))

        def body(n, _):
            cols = pl.ds(pl.multiple_of(n * TILE, TILE), TILE)
            total = dot(hids[0], sd[0, :, cols])
            for i in range(1, nx):
                total = total + dot(hids[i], sd[i, :, cols])
            shared[:, cols] = total
            return 0

        lax.fori_loop(0, width // TILE, body, 0)

    def rs_at(ref, p, d, s, first, count):
        return ref.at[
            col_of(p),
            pl.ds((d * ring + s) * tok + first, count),
            span_of(p),
        ]

    def rs_copy(p, d, s):
        first, count = (d * half, half) if s == 0 else (0, tok)
        return remote(
            rs_at(hbuf, p, d, s, first, count),
            rs_at(rs_recv, p, d, s, first, count),
            rs_sem.at[0, p, d, s],
            rs_sem.at[1, p, d, s],
            at_z(1 - 2 * d),
        )

    def sums_at(p, zi, first, count):
        at = (p % (gu.shape[0] // (nz * tok))) * nz * tok + zi * tok + first
        return slice(at, at + count)

    def sums(p):
        cols = cols_of(p)
        came = ret[col_of(p), :, :, cols].reshape(2 * half_rows, widths[p])
        gu[sums_at(p, 0, 0, nz * tok), : widths[p]] = dot(back[...], came)

    def rs_value(p, zi, first, count, adds):
        total = gu[sums_at(p, zi, first, count), : widths[p]]
        cols = cols_of(p)
        for d, s in adds:
            at = (d * ring + s) * tok + first
            total = total + rs_recv[col_of(p), at : at + count, cols].astype(F32)
        return total

    def rs_step(p, s):
        cols = cols_of(p)
        for d in range(2):
            zi = ring - s if d == 0 else ring + s
            place = (d * ring + s) * tok
            if s > 0:
                with jax.named_scope(f"rswait{p}_{s}"):
                    rs_copy(p, d, s - 1).wait_recv()
            for h in range(2):
                if s > 0 or h == d:
                    adds = ((d, s - 1),) if s > 1 or (s == 1 and h == d) else ()
                    at = place + h * half
                    hbuf[col_of(p), at : at + half, cols] = rs_value(p, zi, h * half, half, adds).astype(BF16)
            rs_copy(p, d, s).start()

    def rs_last(p):
        with jax.named_scope(f"rswait{p}_last"):
            for d in range(2):
                rs_copy(p, d, ring - 1).wait_recv()
        wide = slice(starts[p], starts[p] + widths[p])
        total = rs_value(p, 0, 0, tok, ((0, ring - 1), (1, ring - 1)))
        moe_out[:, wide] = (total + shared[:, wide]).astype(BF16)

    def ret_wait(p):
        with jax.named_scope(f"retwait{p}"):
            r_wait(p, 1)
        sums(p)

    def give_back(p):
        cols = cols_of(p)
        g = col_of(p)
        for j in range(2):
            with jax.named_scope(f"pwait{p}{j}"):
                p_copy(p, j).wait_recv()
            own[g, j, :, cols] = (own[g, j, :, cols].astype(F32) + xback[g, j, :, cols].astype(F32)).astype(BF16)
        for r in order[::-1]:
            r_copy(p, r).start()
        ret[g, :, 0:group, cols] = own[g, :, 0:group, cols]

    for s in range(1, ring):
        with jax.named_scope(f"z0_{s}"):
            for d in range(2):
                meta_copy(d, s - 1).wait_recv()
                if meta_goes(d, s):
                    meta_copy(d, s).start()
            z_forward(0, s)
    z_first(1)
    meta_copy(0, ring - 1).wait_recv()
    for copy in loads[1:]:
        copy.wait()
    with jax.named_scope("tables"):
        for zi in range(nz):
            tables(zi)
    with jax.named_scope("last_z0"):
        last_z(0)
    with jax.named_scope("select0"):
        select(0)
        y_start(0)
    for s in range(1, ring):
        with jax.named_scope(f"z1_{s}"):
            z_forward(1, s)
        with jax.named_scope(f"xfwd0_{s}"):
            x_forward(0, order[(s - 1) * len(order) // ring : s * len(order) // ring])
    with jax.named_scope("xfwd0_rest"):
        x_forward(0, order[(ring - 1) * len(order) // ring :])
    with jax.named_scope("last_z1"):
        last_z(1)
    with jax.named_scope("select1"):
        select(1)
        y_start(1)
    with jax.named_scope("shared_x"):
        for a in range(3):
            shared_x_wait(a, 1)
            for step in range(1, nz):
                shared_z(a, step).start()
    with jax.named_scope("weights"):
        for j in range(2):
            for copy in own_copies(j):
                copy.wait()
            for copy in wide_copies(j):
                copy.wait_recv()
    with jax.named_scope("own_gu0"):
        for j in range(2):
            gate_up(0, 0, j)
    with jax.named_scope("xfwd1"):
        x_forward(1, order)
    with jax.named_scope("shared_z"):
        for a in range(3):
            shared_z_wait(a, 1)
            for d in range(2):
                shared_y(a, d).start()
    for p in range(AHEAD):
        for j in range(2):
            down_copy(j, p).start()
    with jax.named_scope("own_gu1"):
        for j in range(2):
            gate_up(0, 1, j)
            hidden(0, j)
    for j in range(2):
        with jax.named_scope(f"xwait0_{j}"):
            wait_bytes(xrecv.at[0, pl.ds(j * half_rows, half_rows)], x_sem.at[1, 0, j])
        with jax.named_scope("par_gu0"):
            gate_up(1, 0, j)
    with jax.named_scope("mixer"):
        mixer()
    far_rows = 2 * (half_rows - group)
    for g in range(COLS):
        wait_bytes(sendbuf.at[g, pl.ds(0, far_rows)], ys_sem.at[g])
        for d in range(2):
            for s in range(ring):
                for h in range(2):
                    if sends_half(d, s, h):
                        z_copy(g, d, s, h).wait_send()
    for j in range(2):
        with jax.named_scope(f"xwait1_{j}"):
            wait_bytes(xrecv.at[1, pl.ds(j * half_rows, half_rows)], x_sem.at[1, 1, j])
        with jax.named_scope("par_gu1"):
            gate_up(1, 1, j)
            hidden(1, j)

    def downs(p):
        for j in range(2):
            with jax.named_scope(f"wd{p}{j}"):
                down_copy(j, p).wait_recv()
            down(1, p, j)
            p_copy(p, j).start()
            if p + AHEAD < PARTS:
                down_copy(j, p + AHEAD).start()
        for j in range(2):
            down(0, p, j)

    def shared_step(step):
        with jax.named_scope(f"shared{step}"):
            for a in range(3):
                if step == 0:
                    for d in range(2):
                        shared_y(a, d).wait_recv()
                    shared_y2(a).start()
                    for dy in (0, 1, -1):
                        shared_core(a, dy).start()
                if step == 1:
                    shared_y2(a).wait_recv()
                    shared_core(a, 2).start()
            if step == 2:
                shared_expert()

    events = [(when, shared_step, (step,)) for step, when in enumerate(SHARED_AT)]
    for p in range(PARTS):
        start = GAP * starts[p] / (256 * scale)
        full = GAP * widths[p] / (256 * scale)
        events.append((start - LEAD, downs, (p,)))
        events.append((start + full + GIVE, give_back, (p,)))
        come = start + full + GIVE + 3.0 + 6.0 * widths[p] / (256 * scale)
        events.append((come, ret_wait, (p,)))
        for s in range(ring):
            events.append((come + 0.1 + HOP * s, rs_step, (p, s)))
        events.append((max(come + 0.1 + HOP * ring, SHARED_AT[2] + 0.1), rs_last, (p,)))
    for _, act, args in sorted(events, key=lambda e: e[0]):
        act(*args)

    for g in range(COLS):
        for j in range(2):
            wait_bytes(recv.at[g, pl.ds(0, half_rows)], x_sem.at[0, g, j])
    pltpu.make_async_copy(mixed, mix_out, mix_sem.at[2]).wait()
    halo_copy.wait_send()
    for d in range(2):
        for s in range(ring):
            if meta_goes(d, s):
                meta_copy(d, s).wait_send()
    for p in range(PARTS):
        r_wait(p, 0)
        for d in range(2):
            for s in range(ring):
                rs_copy(p, d, s).wait_send()
        for j in range(2):
            p_copy(p, j).wait_send()
            down_copy(j, p).wait_send()
    for j in range(2):
        for copy in wide_copies(j):
            copy.wait_send()
    for a in range(3):
        shared_x_wait(a, 0)
        shared_z_wait(a, 0)
        shared_y2(a).wait_send()
        shared_core_wait(a, 0)
        for d in range(2):
            shared_y(a, d).wait_send()


def fused(dims, moe_input, moe_gain, ids, scores, mix_gain, scale, mix_input, pool, routed, shared):
    nz, ny, nx, tok, cap, width = dims
    peers, ring = ny * NC, nz // 2
    group = nz * cap
    half_rows = peers * group
    rows = 2 * half_rows
    piece = width // COLS
    hid = routed[0].shape[2]
    sh = shared[0].shape[1]
    count = mix_input.shape[0]
    line = np.arange(rows)
    rep = (line[:, None] // group == np.arange(2 * peers)[None, :]).astype(np.float32)
    turn = (line // cap) % nz
    tgt = np.where(turn[:, None] == np.arange(nz)[None, :], (line % cap)[:, None], -1).astype(np.float32)
    vmem = pl.BlockSpec(memory_space=pltpu.VMEM)
    hbm = pl.BlockSpec(memory_space=pl.ANY)
    dma = pltpu.SemaphoreType.DMA
    return pl.pallas_call(
        functools.partial(fused_kernel, dims),
        out_shape=(jax.ShapeDtypeStruct((count, width), BF16), jax.ShapeDtypeStruct((tok, width), BF16)),
        in_specs=[hbm] + [vmem] * 3 + [hbm] * 4 + [vmem] * 2 + [hbm] * 8,
        out_specs=(hbm, vmem),
        scratch_shapes=[
            pltpu.VMEM((COLS, nz * tok, piece), BF16),
            pltpu.VMEM((nz, 16, tok), BF16),
            pltpu.VMEM((rows, nz * tok), BF16),
            pltpu.VMEM((nz * tok, rows), BF16),
            pltpu.VMEM((2, 4, width, hid), BF16),
            pltpu.VMEM((2, 2, hid, width), BF16),
            pltpu.VMEM((COLS, rows, piece), BF16),
            pltpu.VMEM((COLS, rows, piece), BF16),
            pltpu.VMEM((COLS, rows, piece), BF16),
            pltpu.VMEM((16 * half_rows, hid), F32),
            pltpu.VMEM((2, 2, 2, half_rows, hid), BF16),
            pltpu.VMEM((COLS, 2, half_rows, piece), BF16),
            pltpu.VMEM((COLS, 2, half_rows, piece), BF16),
            pltpu.VMEM((COLS, 2, half_rows, piece), BF16),
            pltpu.VMEM((COLS, nz * tok, piece), BF16),
            pltpu.VMEM((tok, width), F32),
            pltpu.VMEM((nx, width, sh), BF16),
            pltpu.VMEM((nx, width, sh), BF16),
            pltpu.VMEM((nx, sh, width), BF16),
            pltpu.VMEM((count, width), BF16),
            pltpu.VMEM((16, width), BF16),
            pltpu.VMEM(pool.shape, BF16),
            pltpu.VMEM((tok, width), BF16),
            pltpu.VMEM((rows, 2 * peers), BF16),
            pltpu.VMEM((2 * peers, rows), BF16),
            pltpu.VMEM((rows, nz), F32),
            pltpu.VMEM((nz, rows), F32),
            pltpu.VMEM((count, width // len(WINDOWS)), BF16),
            pltpu.VMEM((count, width), BF16),
            dma((2, 2, ring)),
            dma((2, COLS, 2, ring, 2)),
            dma((COLS,)),
            dma((COLS, 2, peers)),
            dma((2, COLS, 2)),
            dma((2, PARTS, 2)),
            dma((2, PARTS)),
            dma((2, PARTS, 2, ring)),
            dma((2, 3)),
            dma((2, 2, 2)),
            dma((2, 2, PARTS)),
            dma((2, 3)),
            dma((2, 3, 2)),
            dma((2, 3)),
            dma((2, 3)),
            dma((3, 3)),
            dma((3,)),
            dma((2,)),
            dma((5,)),
        ],
        compiler_params=pltpu.CompilerParams(
            collective_id=0, has_side_effects=True, vmem_limit_bytes=67043328
        ),
    )(
        moe_input,
        moe_gain.reshape(1, width),
        ids.T,
        scores.T,
        jnp.asarray(rep, BF16),
        jnp.asarray(rep.T, BF16),
        jnp.asarray(tgt),
        jnp.asarray(tgt.T),
        mix_gain.reshape(1, width),
        scale.reshape(1, width),
        mix_input,
        pool,
        *routed,
        *shared,
    )


def per_device(
    sizes,
    mix_input,
    mix_gain,
    pool_weight,
    pool_scale,
    moe_input,
    moe_gain,
    expert_ids,
    route_score,
    expert_gate,
    expert_up,
    expert_down,
    shared_gate,
    shared_up,
    shared_down,
):
    nz, ny = sizes
    tok, width = moe_input.shape
    experts = lax.axis_size("ep") * expert_gate.shape[0]
    cap = 3 * tok * expert_ids.shape[1] // (2 * experts)
    dims = (nz, ny, lax.axis_size("tp"), tok, cap, width)
    return fused(
        dims,
        moe_input,
        moe_gain,
        expert_ids,
        route_score,
        mix_gain,
        pool_scale,
        mix_input,
        pool_weight,
        (expert_gate, expert_up, expert_down),
        (shared_gate, shared_up, shared_down),
    )


def solution(mesh, sizes=(NZ, NY)):
    return jax.shard_map(
        functools.partial(per_device, sizes),
        mesh=mesh,
        in_specs=(
            P(("ep", "tp"), None),
            P(),
            P(),
            P(),
            P(("ep", "tp"), None),
            P(),
            P("ep", None),
            P(("ep", "tp"), None),
            P("ep", None, "tp"),
            P("ep", None, "tp"),
            P("ep", "tp", None),
            P(None, "tp"),
            P(None, "tp"),
            P("tp", None),
        ),
        out_specs=(P(("ep", "tp"), None), P(("ep", "tp"), None)),
        check_vma=False,
    )
```

```python
import functools

import jax
import jax.numpy as jnp
import numpy as np
from jax import lax
from jax.experimental import pallas as pl
from jax.experimental.pallas import tpu as pltpu
from jax.sharding import PartitionSpec as P

MESH = pl.DeviceIdType.MESH
F32, BF16 = jnp.float32, jnp.bfloat16
WINDOWS = (2, 4, 8, 16)
RMS_EPS = 1e-06
ROUTED_SCALE = 2.5
NZ, NY, NC = 8, 4, 2
COLS = 2
WIDTHS = (256, 256, 256, 256, 256, 256, 256, 128, 128)
PARTS = len(WIDTHS)
TILE = 256
GAP, HOP, LEAD, GIVE, AHEAD = 7.0, 5.5, 3.0, 1.0, 2
SHARED_AT = (6.5, 16.2, 27.5)


def rms_norm(values, gain_row):
    upcast = values.astype(F32)
    scaled = upcast * lax.rsqrt(jnp.mean(upcast * upcast, axis=-1, keepdims=True) + RMS_EPS)
    return (scaled * gain_row).astype(BF16)


def dot(a, b):
    return jnp.dot(a, b, preferred_element_type=F32)


def fused_kernel(
    dims,
    x_hbm,
    gain_ref,
    ids_ref,
    score_ref,
    rep_hbm,
    rept_hbm,
    tgt_hbm,
    tgtt_hbm,
    mix_gain_ref,
    scale_ref,
    mix_ref,
    pool_ref,
    gate_ref,
    up_ref,
    down_ref,
    sgate_ref,
    sup_ref,
    sdown_ref,
    mix_out,
    moe_out,
    hbuf,
    metab,
    pick,
    back,
    wgu,
    wd,
    sendbuf,
    recv,
    xrecv,
    gu,
    hidb,
    own,
    xback,
    ret,
    rs_recv,
    shared,
    sg,
    su,
    sd,
    mixb,
    halo,
    pool,
    x_ref,
    rep_ref,
    rept_ref,
    tgt_ref,
    tgtt_ref,
    diff,
    mixed,
    m_sem,
    z_sem,
    ys_sem,
    yr_sem,
    x_sem,
    p_sem,
    r_sem,
    rs_sem,
    wl_sem,
    w_sem,
    wd_sem,
    sx_sem,
    sy_sem,
    sz_sem,
    sr_sem,
    sc_sem,
    mix_sem,
    halo_sem,
    in_sem,
):
    nz, ny, nx, tok, cap, width = dims
    ring = nz // 2
    peers = ny * NC
    group = nz * cap
    half_rows = peers * group
    piece = width // COLS
    scale = width // sum(WIDTHS)
    starts = [sum(WIDTHS[:p]) * scale for p in range(PARTS)]
    widths = [w * scale for w in WIDTHS]

    def col_of(p):
        return starts[p] // piece

    def cols_of(p):
        return slice(starts[p] % piece, starts[p] % piece + widths[p])

    def span_of(p):
        return pl.ds(starts[p] % piece, widths[p])
    half = tok // 2
    ep = lax.axis_index("ep")
    tp = lax.axis_index("tp")
    z, q = ep // peers, ep % peers
    y, core = q // NC, q % NC

    def at_z(step):
        return {"ep": ((z + step + nz) % nz) * peers + q}

    def peer_of(dy, dc):
        return ((y + dy + ny) % ny) * NC + (core + dc + NC) % NC

    def at_peer(dy, dc):
        return {"ep": z * peers + peer_of(dy, dc)}

    def at_line(step):
        count = lax.axis_size("ep") * nx
        line = (ep * nx + tp + step + count) % count
        return {"ep": line // nx, "tp": line % nx}

    near = tp + 1 - 2 * (tp % 2)
    far = nx - 1 - tp
    weight_side = ({"tp": near}, {"tp": far})
    token_side = ({"tp": far}, {"tp": near})

    loads = [
        pltpu.make_async_copy(src, dst, in_sem.at[i])
        for i, (src, dst) in enumerate(
            ((x_hbm, x_ref), (rep_hbm, rep_ref), (rept_hbm, rept_ref), (tgt_hbm, tgt_ref), (tgtt_hbm, tgtt_ref))
        )
    ]
    for copy in loads:
        copy.start()

    barrier = pltpu.get_barrier_semaphore()
    greet = [at_z(step) for step in range(1, nz)] + [{"tp": near}, {"tp": far}, {"tp": (tp + 2) % nx}, at_line(1), at_line(-1)]
    greet += [at_peer(r // NC, r % NC) for r in range(1, peers)]
    for device in greet:
        pl.semaphore_signal(barrier, inc=1, device_id=device, device_id_type=MESH)
    with jax.named_scope("barrier"):
        pl.semaphore_wait(barrier, len(greet))

    def remote(src, dst, send, recv_, device):
        return pltpu.make_async_remote_copy(
            src_ref=src, dst_ref=dst, send_sem=send, recv_sem=recv_, device_id=device, device_id_type=MESH
        )

    def wait_bytes(ref, sem):
        pltpu.make_async_copy(ref, ref, sem).wait()

    def wide_copies(j):
        return [
            remote(src.at[j], wgu.at[j, 2 + i], w_sem.at[0, j, i], w_sem.at[1, j, i], weight_side[j])
            for i, src in enumerate((gate_ref, up_ref))
        ]

    def down_copy(j, p):
        cols = pl.ds(starts[p], widths[p])
        return remote(
            down_ref.at[j, :, cols], wd.at[j, 1, :, cols], wd_sem.at[0, j, p], wd_sem.at[1, j, p], weight_side[j]
        )

    def own_copies(j):
        return [
            pltpu.make_async_copy(gate_ref.at[j], wgu.at[j, 0], wl_sem.at[j, 0]),
            pltpu.make_async_copy(up_ref.at[j], wgu.at[j, 1], wl_sem.at[j, 1]),
            pltpu.make_async_copy(down_ref.at[j], wd.at[j, 0], wl_sem.at[j, 2]),
        ]

    for j in range(2):
        for copy in wide_copies(j):
            copy.start()

    loads[0].wait()
    hold = rms_norm(x_ref[...], gain_ref[...])
    for g in range(COLS):
        hbuf[g, 0:tok] = hold[:, g * piece : (g + 1) * piece]

    def meta_copy(d, s):
        src = (-s if d == 0 else s) % nz
        dst = (-s - 1 if d == 0 else s + 1) % nz
        return remote(metab.at[src], metab.at[dst], m_sem.at[0, d, s], m_sem.at[1, d, s], at_z(1 - 2 * d))

    def z_copy(g, d, s, h):
        src = (-s if d == 0 else s) % nz
        dst = (-s - 1 if d == 0 else s + 1) % nz
        return remote(
            hbuf.at[g, pl.ds(src * tok + h * half, half)],
            hbuf.at[g, pl.ds(dst * tok + h * half, half)],
            z_sem.at[0, g, d, s, h],
            z_sem.at[1, g, d, s, h],
            at_z(1 - 2 * d),
        )

    def sends_half(d, s, h):
        return s < ring - 1 or h == d

    def meta_goes(d, s):
        return s < ring - 1 or d == 0

    def z_first(g):
        for h in range(2):
            for d in range(2):
                z_copy(g, d, 0, h).start()

    def z_forward(g, s):
        for h in range(2):
            for d in range(2):
                z_copy(g, d, s - 1, h).wait_recv()
                if sends_half(d, s, h):
                    z_copy(g, d, s, h).start()

    def last_z(g):
        for d in range(2):
            z_copy(g, d, ring - 1, d).wait_recv()

    z_first(0)
    my_ids = ids_ref[:, pl.ds(pl.multiple_of(tp * tok, tok), tok)].astype(F32)
    scores = score_ref[...]
    route = scores / jnp.sum(scores, axis=0, keepdims=True) * ROUTED_SCALE
    metab[0] = jnp.concatenate([my_ids, route, jnp.zeros((8, tok), F32)], axis=0).astype(BF16)
    for d in range(2):
        meta_copy(d, 0).start()

    for j in range(2):
        for copy in own_copies(j):
            copy.start()
    pieces = ((sgate_ref, sg, sg.shape[1] // peers), (sup_ref, su, su.shape[1] // peers), (sdown_ref, sd, sd.shape[1] // peers))
    shared_own = [pltpu.make_async_copy(src, dst.at[0], sc_sem.at[0, a]) for a, (src, dst, _) in enumerate(pieces)]
    mix_copies = [
        pltpu.make_async_copy(mix_ref, mixb, mix_sem.at[0]),
        pltpu.make_async_copy(pool_ref, pool, mix_sem.at[1]),
    ]
    reach = halo.shape[0]
    halo_copy = remote(
        mix_ref.at[pl.ds(mix_ref.shape[0] - reach, reach)], halo, halo_sem.at[0], halo_sem.at[1], at_line(1)
    )
    for copy in shared_own + mix_copies + [halo_copy]:
        copy.start()

    def piece_at(dst, size, which):
        return dst.at[pl.ds(1, nx - 1), pl.ds(which * size, size)]

    def crumb(a):
        _, dst, size = pieces[a]
        if a < 2:
            small = size // nz
            return (pl.ds(q * size + z * small, small),)
        small = dst.shape[2] // nz
        return (pl.ds(q * size, size), pl.ds(pl.multiple_of(z * small, small), small))

    def crumbs(a, count):
        _, dst, size = pieces[a]
        if a < 2:
            return dst.at[pl.ds(1, nx - 1), pl.ds(0, count * (size // nz))]
        return dst.at[pl.ds(1, nx - 1), pl.ds(0, size), pl.ds(0, count * (dst.shape[2] // nz))]

    def shared_x(a, step):
        src, dst, _ = pieces[a]
        at = crumb(a)
        return remote(
            src.at[at], dst.at[(nx - step, *at)], sx_sem.at[0, a], sx_sem.at[1, a], {"tp": (tp + step) % nx}
        )

    def shared_x_wait(a, side):
        wait_bytes(crumbs(a, 1), sx_sem.at[side, a])

    def shared_z(a, step):
        _, dst, _ = pieces[a]
        ref = dst.at[(pl.ds(1, nx - 1), *crumb(a))]
        return remote(ref, ref, sr_sem.at[0, a], sr_sem.at[1, a], at_z(step))

    def shared_z_wait(a, side):
        wait_bytes(crumbs(a, nz - 1), sr_sem.at[side, a])

    def shared_y(a, d):
        _, dst, size = pieces[a]
        ref = piece_at(dst, size, q)
        return remote(ref, ref, sy_sem.at[0, a, d], sy_sem.at[1, a, d], at_peer(1 - 2 * d, 0))

    def shared_y2(a):
        d = a % 2
        _, dst, size = pieces[a]
        ref = piece_at(dst, size, peer_of(2 * d - 1, 0))
        return remote(ref, ref, sz_sem.at[0, a], sz_sem.at[1, a], at_peer(1 - 2 * d, 0))

    def shared_core(a, dy):
        _, dst, size = pieces[a]
        ref = piece_at(dst, size, peer_of(dy, 0))
        return remote(ref, ref, sc_sem.at[1, a], sc_sem.at[2, a], at_peer(0, 1))

    def shared_core_wait(a, side):
        _, dst, size = pieces[a]
        wait_bytes(dst.at[pl.ds(1, nx - 1), pl.ds(0, ny * size)], sc_sem.at[1 + side, a])

    for a in range(3):
        for step in (1, nx - 1, 2):
            shared_x(a, step).start()

    before = lax.broadcasted_iota(jnp.int32, (tok, tok), 0) < lax.broadcasted_iota(jnp.int32, (tok, tok), 1)
    upper = before.astype(F32).astype(BF16)
    line = lax.broadcasted_iota(jnp.int32, (2 * peers, tok), 0)
    their_core = (core + line % NC) % NC
    their_y = (y + (line % peers) // NC) % ny
    names = (2 * (z * peers + their_y * NC + their_core) + line // peers).astype(F32)

    def tables(zi):
        block = metab[zi].astype(F32)
        named = jnp.zeros((2 * peers, tok), F32)
        weight = jnp.zeros((2 * peers, tok), F32)
        for k in range(4):
            same = (block[k : k + 1] == names).astype(F32)
            named = named + same
            weight = weight + same * block[4 + k : 5 + k]
        rank = dot(named.astype(BF16), upper)
        rank = jnp.where(named > 0.5, rank, -2.0)
        spread = dot(rep_ref[...], rank.astype(BF16))
        pick[:, zi * tok : (zi + 1) * tok] = (spread == tgt_ref[:, zi : zi + 1]).astype(F32).astype(BF16)
        padding = jnp.zeros((tok - 4 * peers, tok), F32)
        turned = jnp.transpose(jnp.concatenate([rank, weight, padding], axis=0))
        spread_t = dot(turned[:, : 2 * peers].astype(BF16), rept_ref[...])
        weight_t = dot(turned[:, 2 * peers : 4 * peers].astype(BF16), rept_ref[...])
        back[zi * tok : (zi + 1) * tok] = jnp.where(spread_t == tgtt_ref[zi : zi + 1], weight_t, 0.0).astype(BF16)

    def select(g):
        def body(n, _):
            cols = pl.ds(pl.multiple_of(n * TILE, TILE), TILE)
            sendbuf[g, :, cols] = dot(pick[...], hbuf[g, :, cols]).astype(BF16)
            return 0

        lax.fori_loop(0, piece // TILE, body, 0)
        for j in range(2):
            recv[g, j * half_rows : j * half_rows + group] = sendbuf[g, j * half_rows : j * half_rows + group]

    def y_copy(g, j, r):
        part = pl.ds(j * half_rows + r * group, group)
        return remote(
            sendbuf.at[g, part], recv.at[g, part], ys_sem.at[g], yr_sem.at[g, j, r], at_peer(r // NC, r % NC)
        )

    def x_copy(g, j, r):
        part = pl.ds(j * half_rows + r * group, group)
        return remote(recv.at[g, part], xrecv.at[g, part], x_sem.at[0, g, j], x_sem.at[1, g, j], token_side[j])

    order = list(range(1, peers))
    order.sort(key=lambda r: min(r // NC, ny - r // NC))

    def y_start(g):
        for r in order[::-1]:
            for j in range(2):
                y_copy(g, j, r).start()
        for j in range(2):
            x_copy(g, j, 0).start()

    def x_forward(g, some):
        for r in some:
            for j in range(2):
                y_copy(g, j, r).wait_recv()
                x_copy(g, j, r).start()

    def gate_up(which, g, j):
        src = (recv, xrecv)[which]

        def body(n, _):
            part = dot(src[g, j * half_rows : (j + 1) * half_rows], wgu[j, n, g * piece : (g + 1) * piece])
            at = pl.ds(pl.multiple_of(((which * 2 + j) * 4 + n) * half_rows, half_rows), half_rows)
            if g == 0:
                gu[at] = part
            else:
                gu[at] = gu[at] + part
            return 0

        lax.fori_loop(0, 4, body, 0)

    def hidden(which, j):
        for i in range(2):
            at = ((which * 2 + j) * 4 + i * 2) * half_rows
            gate = gu[at : at + half_rows]
            up = gu[at + half_rows : at + 2 * half_rows]
            hidb[which, j, i] = (gate / (1.0 + jnp.exp(-gate)) * up).astype(BF16)

    def down(which, p, j):
        wide = slice(starts[p], starts[p] + widths[p])
        val = dot(hidb[which, j, 0], wd[j, 0, :, wide]) + dot(hidb[which, j, 1], wd[j, 1, :, wide])
        if which == 0:
            own[col_of(p), j, :, cols_of(p)] = val.astype(BF16)
        else:
            sendbuf[col_of(p), j * half_rows : (j + 1) * half_rows, cols_of(p)] = val.astype(BF16)

    def at_part(ref, p, which, rows_at):
        return ref.at[col_of(p), which, rows_at, span_of(p)]

    def p_copy(p, j):
        return remote(
            sendbuf.at[col_of(p), pl.ds(j * half_rows, half_rows), span_of(p)],
            at_part(xback, p, j, pl.ds(0, half_rows)),
            p_sem.at[0, p, j],
            p_sem.at[1, p, j],
            token_side[j],
        )

    def r_copy(p, r):
        rows_at, both = pl.ds(r * group, group), pl.ds(0, 2)
        return remote(
            at_part(own, p, both, rows_at),
            at_part(ret, p, both, rows_at),
            r_sem.at[0, p],
            r_sem.at[1, p],
            at_peer(-(r // NC), -(r % NC)),
        )

    def r_wait(p, side):
        wait_bytes(at_part(ret, p, pl.ds(0, 2), pl.ds(0, half_rows - group)), r_sem.at[side, p])

    def mixer():
        for copy in mix_copies:
            copy.wait()
        halo_copy.wait_recv()
        count = mixb.shape[0]
        lead = jnp.where(ep * nx + tp > 0, 1.0, 0.0)
        body_in = mixb[...].astype(F32)
        halo_in = halo[...].astype(F32) * lead
        scales = [
            lax.rsqrt(jnp.mean(v * v, axis=-1, keepdims=True) + RMS_EPS) for v in (halo_in, body_in)
        ]
        position = (ep * nx + tp) * count + lax.broadcasted_iota(jnp.int32, (count, 1), 0)
        span_width = width // len(WINDOWS)
        for g, span in enumerate(WINDOWS):
            counts = jnp.minimum(position + 1, span).astype(F32)
            for n in range(span_width // TILE):
                cols = slice(g * span_width + n * TILE, g * span_width + (n + 1) * TILE)
                gain = mix_gain_ref[:, cols]
                top = (halo[:, cols].astype(F32) * lead * scales[0] * gain).astype(BF16).astype(F32)
                rest = (mixb[:, cols].astype(F32) * scales[1] * gain).astype(BF16).astype(F32)
                total = jnp.concatenate([top, rest], axis=0)
                step = 1
                while step < span:
                    total = total + pltpu.roll(total, step, 0)
                    step *= 2
                diff[:, n * TILE : (n + 1) * TILE] = (total[reach:] / counts - rest).astype(BF16)
            cols = slice(g * span_width, (g + 1) * span_width)
            mixed[:, cols] = (dot(diff[...], pool[g]) * scale_ref[:, cols]).astype(BF16)
        pltpu.make_async_copy(mixed, mix_out, mix_sem.at[2]).start()

    def shared_expert():
        for a in range(3):
            shared_own[a].wait()
            shared_core_wait(a, 1)
        again = rms_norm(x_ref[...], gain_ref[...])
        tokens = [again[:, g * piece : (g + 1) * piece] for g in range(COLS)]
        hids = []
        for i in range(nx):
            gate = dot(tokens[0], sg[i, :piece]) + dot(tokens[1], sg[i, piece:])
            up = dot(tokens[0], su[i, :piece]) + dot(tokens[1], su[i, piece:])
            hids.append((gate / (1.0 + jnp.exp(-gate)) * up).astype(BF16))

        def body(n, _):
            cols = pl.ds(pl.multiple_of(n * TILE, TILE), TILE)
            total = dot(hids[0], sd[0, :, cols])
            for i in range(1, nx):
                total = total + dot(hids[i], sd[i, :, cols])
            shared[:, cols] = total
            return 0

        lax.fori_loop(0, width // TILE, body, 0)

    def rs_at(ref, p, d, s, first, count):
        return ref.at[
            col_of(p),
            pl.ds((d * ring + s) * tok + first, count),
            span_of(p),
        ]

    def rs_copy(p, d, s):
        first, count = (d * half, half) if s == 0 else (0, tok)
        return remote(
            rs_at(hbuf, p, d, s, first, count),
            rs_at(rs_recv, p, d, s, first, count),
            rs_sem.at[0, p, d, s],
            rs_sem.at[1, p, d, s],
            at_z(1 - 2 * d),
        )

    def sums_at(p, zi, first, count):
        at = (p % (gu.shape[0] // (nz * tok))) * nz * tok + zi * tok + first
        return slice(at, at + count)

    def sums(p):
        cols = cols_of(p)
        came = ret[col_of(p), :, :, cols].reshape(2 * half_rows, widths[p])
        gu[sums_at(p, 0, 0, nz * tok), : widths[p]] = dot(back[...], came)

    def rs_value(p, zi, first, count, adds):
        total = gu[sums_at(p, zi, first, count), : widths[p]]
        cols = cols_of(p)
        for d, s in adds:
            at = (d * ring + s) * tok + first
            total = total + rs_recv[col_of(p), at : at + count, cols].astype(F32)
        return total

    def rs_step(p, s):
        cols = cols_of(p)
        for d in range(2):
            zi = ring - s if d == 0 else ring + s
            place = (d * ring + s) * tok
            if s > 0:
                with jax.named_scope(f"rswait{p}_{s}"):
                    rs_copy(p, d, s - 1).wait_recv()
            for h in range(2):
                if s > 0 or h == d:
                    adds = ((d, s - 1),) if s > 1 or (s == 1 and h == d) else ()
                    at = place + h * half
                    hbuf[col_of(p), at : at + half, cols] = rs_value(p, zi, h * half, half, adds).astype(BF16)
            rs_copy(p, d, s).start()

    def rs_last(p):
        with jax.named_scope(f"rswait{p}_last"):
            for d in range(2):
                rs_copy(p, d, ring - 1).wait_recv()
        wide = slice(starts[p], starts[p] + widths[p])
        total = rs_value(p, 0, 0, tok, ((0, ring - 1), (1, ring - 1)))
        moe_out[:, wide] = (total + shared[:, wide]).astype(BF16)

    def ret_wait(p):
        with jax.named_scope(f"retwait{p}"):
            r_wait(p, 1)
        sums(p)

    def give_back(p):
        cols = cols_of(p)
        g = col_of(p)
        for j in range(2):
            with jax.named_scope(f"pwait{p}{j}"):
                p_copy(p, j).wait_recv()
            own[g, j, :, cols] = (own[g, j, :, cols].astype(F32) + xback[g, j, :, cols].astype(F32)).astype(BF16)
        for r in order[::-1]:
            r_copy(p, r).start()
        ret[g, :, 0:group, cols] = own[g, :, 0:group, cols]

    for s in range(1, ring):
        with jax.named_scope(f"z0_{s}"):
            for d in range(2):
                meta_copy(d, s - 1).wait_recv()
                if meta_goes(d, s):
                    meta_copy(d, s).start()
            z_forward(0, s)
    z_first(1)
    meta_copy(0, ring - 1).wait_recv()
    for copy in loads[1:]:
        copy.wait()
    with jax.named_scope("tables"):
        for zi in range(nz):
            tables(zi)
    with jax.named_scope("last_z0"):
        last_z(0)
    with jax.named_scope("select0"):
        select(0)
        y_start(0)
    for s in range(1, ring):
        with jax.named_scope(f"z1_{s}"):
            z_forward(1, s)
        with jax.named_scope(f"xfwd0_{s}"):
            x_forward(0, order[(s - 1) * len(order) // ring : s * len(order) // ring])
    with jax.named_scope("xfwd0_rest"):
        x_forward(0, order[(ring - 1) * len(order) // ring :])
    with jax.named_scope("last_z1"):
        last_z(1)
    with jax.named_scope("select1"):
        select(1)
        y_start(1)
    with jax.named_scope("shared_x"):
        for a in range(3):
            shared_x_wait(a, 1)
            for step in range(1, nz):
                shared_z(a, step).start()
    with jax.named_scope("weights"):
        for j in range(2):
            for copy in own_copies(j):
                copy.wait()
            for copy in wide_copies(j):
                copy.wait_recv()
    with jax.named_scope("own_gu0"):
        for j in range(2):
            gate_up(0, 0, j)
    with jax.named_scope("xfwd1"):
        x_forward(1, order)
    with jax.named_scope("shared_z"):
        for a in range(3):
            shared_z_wait(a, 1)
            for d in range(2):
                shared_y(a, d).start()
    for p in range(AHEAD):
        for j in range(2):
            down_copy(j, p).start()
    with jax.named_scope("own_gu1"):
        for j in range(2):
            gate_up(0, 1, j)
            hidden(0, j)
    for j in range(2):
        with jax.named_scope(f"xwait0_{j}"):
            wait_bytes(xrecv.at[0, pl.ds(j * half_rows, half_rows)], x_sem.at[1, 0, j])
        with jax.named_scope("par_gu0"):
            gate_up(1, 0, j)
    with jax.named_scope("mixer"):
        mixer()
    far_rows = 2 * (half_rows - group)
    for g in range(COLS):
        wait_bytes(sendbuf.at[g, pl.ds(0, far_rows)], ys_sem.at[g])
        for d in range(2):
            for s in range(ring):
                for h in range(2):
                    if sends_half(d, s, h):
                        z_copy(g, d, s, h).wait_send()
    for j in range(2):
        with jax.named_scope(f"xwait1_{j}"):
            wait_bytes(xrecv.at[1, pl.ds(j * half_rows, half_rows)], x_sem.at[1, 1, j])
        with jax.named_scope("par_gu1"):
            gate_up(1, 1, j)
            hidden(1, j)

    def downs(p):
        for j in range(2):
            with jax.named_scope(f"wd{p}{j}"):
                down_copy(j, p).wait_recv()
            down(1, p, j)
            p_copy(p, j).start()
            if p + AHEAD < PARTS:
                down_copy(j, p + AHEAD).start()
        for j in range(2):
            down(0, p, j)

    def shared_step(step):
        with jax.named_scope(f"shared{step}"):
            for a in range(3):
                if step == 0:
                    for d in range(2):
                        shared_y(a, d).wait_recv()
                    shared_y2(a).start()
                    for dy in (0, 1, -1):
                        shared_core(a, dy).start()
                if step == 1:
                    shared_y2(a).wait_recv()
                    shared_core(a, 2).start()
            if step == 2:
                shared_expert()

    events = [(when, shared_step, (step,)) for step, when in enumerate(SHARED_AT)]
    for p in range(PARTS):
        start = GAP * starts[p] / (256 * scale)
        full = GAP * widths[p] / (256 * scale)
        events.append((start - LEAD, downs, (p,)))
        events.append((start + full + GIVE, give_back, (p,)))
        come = start + full + GIVE + 3.0 + 6.0 * widths[p] / (256 * scale)
        events.append((come, ret_wait, (p,)))
        for s in range(ring):
            events.append((come + 0.1 + HOP * s, rs_step, (p, s)))
        events.append((max(come + 0.1 + HOP * ring, SHARED_AT[2] + 0.1), rs_last, (p,)))
    for _, act, args in sorted(events, key=lambda e: e[0]):
        act(*args)

    for g in range(COLS):
        for j in range(2):
            wait_bytes(recv.at[g, pl.ds(0, half_rows)], x_sem.at[0, g, j])
    pltpu.make_async_copy(mixed, mix_out, mix_sem.at[2]).wait()
    halo_copy.wait_send()
    for d in range(2):
        for s in range(ring):
            if meta_goes(d, s):
                meta_copy(d, s).wait_send()
    for p in range(PARTS):
        r_wait(p, 0)
        for d in range(2):
            for s in range(ring):
                rs_copy(p, d, s).wait_send()
        for j in range(2):
            p_copy(p, j).wait_send()
            down_copy(j, p).wait_send()
    for j in range(2):
        for copy in wide_copies(j):
            copy.wait_send()
    for a in range(3):
        shared_x_wait(a, 0)
        shared_z_wait(a, 0)
        shared_y2(a).wait_send()
        shared_core_wait(a, 0)
        for d in range(2):
            shared_y(a, d).wait_send()


def fused(dims, moe_input, moe_gain, ids, scores, mix_gain, scale, mix_input, pool, routed, shared):
    nz, ny, nx, tok, cap, width = dims
    peers, ring = ny * NC, nz // 2
    group = nz * cap
    half_rows = peers * group
    rows = 2 * half_rows
    piece = width // COLS
    hid = routed[0].shape[2]
    sh = shared[0].shape[1]
    count = mix_input.shape[0]
    line = np.arange(rows)
    rep = (line[:, None] // group == np.arange(2 * peers)[None, :]).astype(np.float32)
    turn = (line // cap) % nz
    tgt = np.where(turn[:, None] == np.arange(nz)[None, :], (line % cap)[:, None], -1).astype(np.float32)
    vmem = pl.BlockSpec(memory_space=pltpu.VMEM)
    hbm = pl.BlockSpec(memory_space=pl.ANY)
    dma = pltpu.SemaphoreType.DMA
    return pl.pallas_call(
        functools.partial(fused_kernel, dims),
        out_shape=(jax.ShapeDtypeStruct((count, width), BF16), jax.ShapeDtypeStruct((tok, width), BF16)),
        in_specs=[hbm] + [vmem] * 3 + [hbm] * 4 + [vmem] * 2 + [hbm] * 8,
        out_specs=(hbm, vmem),
        scratch_shapes=[
            pltpu.VMEM((COLS, nz * tok, piece), BF16),
            pltpu.VMEM((nz, 16, tok), BF16),
            pltpu.VMEM((rows, nz * tok), BF16),
            pltpu.VMEM((nz * tok, rows), BF16),
            pltpu.VMEM((2, 4, width, hid), BF16),
            pltpu.VMEM((2, 2, hid, width), BF16),
            pltpu.VMEM((COLS, rows, piece), BF16),
            pltpu.VMEM((COLS, rows, piece), BF16),
            pltpu.VMEM((COLS, rows, piece), BF16),
            pltpu.VMEM((16 * half_rows, hid), F32),
            pltpu.VMEM((2, 2, 2, half_rows, hid), BF16),
            pltpu.VMEM((COLS, 2, half_rows, piece), BF16),
            pltpu.VMEM((COLS, 2, half_rows, piece), BF16),
            pltpu.VMEM((COLS, 2, half_rows, piece), BF16),
            pltpu.VMEM((COLS, nz * tok, piece), BF16),
            pltpu.VMEM((tok, width), F32),
            pltpu.VMEM((nx, width, sh), BF16),
            pltpu.VMEM((nx, width, sh), BF16),
            pltpu.VMEM((nx, sh, width), BF16),
            pltpu.VMEM((count, width), BF16),
            pltpu.VMEM((16, width), BF16),
            pltpu.VMEM(pool.shape, BF16),
            pltpu.VMEM((tok, width), BF16),
            pltpu.VMEM((rows, 2 * peers), BF16),
            pltpu.VMEM((2 * peers, rows), BF16),
            pltpu.VMEM((rows, nz), F32),
            pltpu.VMEM((nz, rows), F32),
            pltpu.VMEM((count, width // len(WINDOWS)), BF16),
            pltpu.VMEM((count, width), BF16),
            dma((2, 2, ring)),
            dma((2, COLS, 2, ring, 2)),
            dma((COLS,)),
            dma((COLS, 2, peers)),
            dma((2, COLS, 2)),
            dma((2, PARTS, 2)),
            dma((2, PARTS)),
            dma((2, PARTS, 2, ring)),
            dma((2, 3)),
            dma((2, 2, 2)),
            dma((2, 2, PARTS)),
            dma((2, 3)),
            dma((2, 3, 2)),
            dma((2, 3)),
            dma((2, 3)),
            dma((3, 3)),
            dma((3,)),
            dma((2,)),
            dma((5,)),
        ],
        compiler_params=pltpu.CompilerParams(
            collective_id=0, has_side_effects=True, vmem_limit_bytes=67043328
        ),
    )(
        moe_input,
        moe_gain.reshape(1, width),
        ids.T,
        scores.T,
        jnp.asarray(rep, BF16),
        jnp.asarray(rep.T, BF16),
        jnp.asarray(tgt),
        jnp.asarray(tgt.T),
        mix_gain.reshape(1, width),
        scale.reshape(1, width),
        mix_input,
        pool,
        *routed,
        *shared,
    )


def hand_over_kernel(mix_in, moe_in, mix_out, moe_out, mix_buf, moe_buf, in_sem, out_sem):
    pairs = ((mix_in, mix_buf, mix_out), (moe_in, moe_buf, moe_out))
    steps = []
    for src, buf, dst in pairs:
        for at in range(0, src.shape[0], 64):
            rows = pl.ds(at, 64)
            i = len(steps)
            steps.append(
                (
                    pltpu.make_async_copy(src.at[rows], buf.at[rows], in_sem.at[i]),
                    pltpu.make_async_copy(buf.at[rows], dst.at[rows], out_sem.at[i]),
                )
            )
    for come, _ in steps:
        come.start()
    for come, go in steps:
        come.wait()
        go.start()
    for _, go in steps:
        go.wait()


def hand_over(mix, moe):
    hbm = pl.BlockSpec(memory_space=pl.ANY)
    count = (mix.shape[0] + moe.shape[0]) // 64
    return pl.pallas_call(
        hand_over_kernel,
        out_shape=(jax.ShapeDtypeStruct(mix.shape, BF16), jax.ShapeDtypeStruct(moe.shape, BF16)),
        in_specs=[hbm, hbm],
        out_specs=(hbm, hbm),
        scratch_shapes=[
            pltpu.VMEM(mix.shape, BF16),
            pltpu.VMEM(moe.shape, BF16),
            pltpu.SemaphoreType.DMA((count,)),
            pltpu.SemaphoreType.DMA((count,)),
        ],
    )(mix, moe)


def per_device(
    sizes,
    mix_input,
    mix_gain,
    pool_weight,
    pool_scale,
    moe_input,
    moe_gain,
    expert_ids,
    route_score,
    expert_gate,
    expert_up,
    expert_down,
    shared_gate,
    shared_up,
    shared_down,
):
    nz, ny = sizes
    tok, width = moe_input.shape
    experts = lax.axis_size("ep") * expert_gate.shape[0]
    cap = 3 * tok * expert_ids.shape[1] // (2 * experts)
    dims = (nz, ny, lax.axis_size("tp"), tok, cap, width)
    mixed, routed_out = fused(
        dims,
        moe_input,
        moe_gain,
        expert_ids,
        route_score,
        mix_gain,
        pool_scale,
        mix_input,
        pool_weight,
        (expert_gate, expert_up, expert_down),
        (shared_gate, shared_up, shared_down),
    )
    return hand_over(mixed, routed_out)


def solution(mesh, sizes=(NZ, NY)):
    return jax.shard_map(
        functools.partial(per_device, sizes),
        mesh=mesh,
        in_specs=(
            P(("ep", "tp"), None),
            P(),
            P(),
            P(),
            P(("ep", "tp"), None),
            P(),
            P("ep", None),
            P(("ep", "tp"), None),
            P("ep", None, "tp"),
            P("ep", None, "tp"),
            P("ep", "tp", None),
            P(None, "tp"),
            P(None, "tp"),
            P("tp", None),
        ),
        out_specs=(P(("ep", "tp"), None), P(("ep", "tp"), None)),
        check_vma=False,
    )
```
